256 devices in a mesh: grp: 2 (over y), kv: 32 (over z, core), tp: 4 (over x).
Axes of the slice: x: 4, y: 2, z: 16, core: 2. Of those that a mesh axis runs over, the one named last changes fastest.
The devices are a block of a 4x16x16 slice.
Arguments:
- tokens: bfloat16 [1408, 6, 4096], P(('grp', 'kv')), parts along dimension 0, may hold values from -6 to 6
- norm_gain: bfloat16 [4096], replicated, may hold values from 0.099609375 to 1.8984375
- w_query: bfloat16 [4096, 2048], P('kv', 'tp'), may hold values from -0.09375 to 0.09375
- w_key: bfloat16 [4096, 2048], P('kv', 'tp'), may hold values from -0.09375 to 0.09375
- w_value: bfloat16 [4096, 2048], P('kv', 'tp'), may hold values from -0.09375 to 0.09375
- w_igate: bfloat16 [4096, 16], P(None, 'tp'), may hold values from -0.09375 to 0.09375
- w_fgate: bfloat16 [4096, 16], P(None, 'tp'), may hold values from -0.09375 to 0.09375
- igate_bias: float32 [16], P('tp'), may hold values from -2 to 2
- fgate_bias: float32 [16], P('tp'), may hold values from 0.5 to 6
- head_gain: bfloat16 [2048], P('tp'), may hold values from 0.099609375 to 1.8984375
- w_out: bfloat16 [2048, 4096], P('tp', 'kv'), may hold values from -0.125 to 0.125
- state_matrix: float32 [1408, 16, 128, 128], P(('grp', 'kv'), 'tp'), parts along dimension 0, may hold values from -1.5 to 1.5
- state_norm: float32 [1408, 16, 128], P(('grp', 'kv'), 'tp'), parts along dimension 0, may hold values from -4 to 4
- state_max: float32 [1408, 16], P(('grp', 'kv'), 'tp'), parts along dimension 0, may hold values from -4 to 4
- prior_keys: bfloat16 [1408, 6, 2048], P(('grp', 'kv'), None, 'tp'), parts along dimension 0, may hold values from -6 to 6
- prior_values: bfloat16 [1408, 6, 2048], P(('grp', 'kv'), None, 'tp'), parts along dimension 0, may hold values from -6 to 6
- prior_igate: float32 [1408, 6, 16], P(('grp', 'kv'), None, 'tp'), parts along dimension 0, may hold values from -4 to 4
- prior_fgate: float32 [1408, 6, 16], P(('grp', 'kv'), None, 'tp'), parts along dimension 0, may hold values from 0 to 5
- accepted: int32 [1408], P(('grp', 'kv')), parts along dimension 0, may hold values from 0 to 6
Outputs:
- mixed: float32 [1408, 6, 4096], P(('grp', 'kv'), None, 'tp'), parts along dimension 0
- new_matrix: float32 [1408, 16, 128, 128], P(('grp', 'kv'), 'tp'), parts along dimension 0
- new_norm: float32 [1408, 16, 128], P(('grp', 'kv'), 'tp'), parts along dimension 0
- new_max: float32 [1408, 16], P(('grp', 'kv'), 'tp'), parts along dimension 0
The draws below stay inside these ranges and needn't reach their ends.
There are 2 independent parts, one for each index of `grp`. The reference program is written for one: setup_inputs(seed, part) draws one part's arguments, and reference() takes and returns one part's arrays. A program takes and returns all parts, laid end to end along the dimension named above; an argument that names none is the same for every part. Nothing has to cross between parts.
Inputs may be any that keep to these rules, and one draw needn't show every extreme that they name: `accepted`: how many of the 6 proposals of the last step were kept, from the first on.
All inputs are finite; a program needn't handle non-finite values.
Results may differ from the reference program's by a relative error of at most 0.019.
Values may be sent and summed in bfloat16 or wider, within the bound.
A program may use at most 128 MiB of HBM per device.

```python
import jax
import jax.numpy as jnp
from jax import lax

D = 4096
HEADS = 16
DK = 128
DV = 128
PROP = 6
SEQS = 704


def with_ends(drawn, own_key, low, high):
    longest = drawn.shape.index(max(drawn.shape))
    spots = []
    for shift in (0, 1):
        where = [jax.random.randint(jax.random.fold_in(own_key, axis), (), 0, length) for axis, length in enumerate(drawn.shape)]
        where[longest] = (where[longest] + shift) % drawn.shape[longest]
        spots.append(tuple(where))
    return drawn.at[spots[0]].set(low).at[spots[1]].set(high)


def block_scale(own_key, shape, shards, smallest, top_value):
    level, own = 1.0, jax.random.fold_in(own_key, 6)
    for axis_at, shards_of in shards:
        draws = jnp.exp(jax.random.uniform(jax.random.fold_in(own, axis_at), (shards_of,), jnp.float32, smallest / len(shards), top_value / len(shards)))
        level = level * jnp.repeat(draws, shape[axis_at] // shards_of).reshape([-1 if axis == axis_at else 1 for axis in range(len(shape))])
    return level


def bell_draw(stream_key, shape, deviation, limit, pieces=(), kind=jnp.bfloat16):
    result = jax.random.normal(stream_key, shape, jnp.float32) * deviation
    if len(pieces) > 0:
        result = block_scale(stream_key, shape, pieces, -0.22, 0.18) * result
    return jnp.clip(result, min=-limit, max=limit).astype(kind)


def setup_inputs(seed: int = 0, part: int = 0) -> dict:
    key_of = jax.random.split(jax.random.key(seed), 20)
    part_splits = jax.random.split(jax.random.fold_in(key_of[19], part), 20)
    tokens = bell_draw(part_splits[0], (SEQS, PROP, D), 1.0, 6.0, ((0, 32),))
    norm_gain = jnp.clip(1.0 + 0.18 * jax.random.normal(key_of[1], (D,), jnp.float32), 0.099609375, 1.8984375).astype(jnp.bfloat16)
    w_query = bell_draw(key_of[2], (D, HEADS * DK), D ** -0.5, 0.09375, ((0, 32), (1, 4)))
    w_key = bell_draw(key_of[3], (D, HEADS * DK), D ** -0.5, 0.09375, ((0, 32), (1, 4)))
    w_value = bell_draw(key_of[4], (D, HEADS * DV), D ** -0.5, 0.09375, ((0, 32), (1, 4)))
    w_igate = bell_draw(key_of[5], (D, HEADS), D ** -0.5, 0.09375, ((1, 4),))
    w_fgate = bell_draw(key_of[6], (D, HEADS), D ** -0.5, 0.09375, ((1, 4),))
    igate_bias = jnp.clip(jax.random.uniform(key_of[7], (HEADS,), jnp.float32, -2.0, 2.0) * block_scale(key_of[7], (HEADS,), ((0, 4),), -0.4, 0.0), -2.0, 2.0)
    fgate_bias = jnp.clip(0.5 + 5.5 * jax.random.uniform(key_of[8], (HEADS,), jnp.float32) ** block_scale(key_of[8], (HEADS,), ((0, 4),), -0.2, 0.2), 0.5, 6.0)
    head_gain = jnp.clip(1.0 + 0.18 * jax.random.normal(key_of[9], (HEADS * DV,), jnp.float32), 0.099609375, 1.8984375).astype(jnp.bfloat16)
    w_out = bell_draw(key_of[10], (HEADS * DV, D), (HEADS * DV) ** -0.5, 0.125, ((0, 4), (1, 32)))
    state_matrix = bell_draw(part_splits[11], (SEQS, HEADS, DK, DV), 0.1, 1.5, ((0, 32), (1, 4)), jnp.float32)
    state_norm = bell_draw(part_splits[12], (SEQS, HEADS, DK), 0.3, 4.0, ((0, 32), (1, 4)), jnp.float32)
    state_max = bell_draw(part_splits[13], (SEQS, HEADS), 1.0, 4.0, ((0, 32), (1, 4)), jnp.float32)
    prior_keys = bell_draw(part_splits[14], (SEQS, PROP, HEADS * DK), 1.0, 6.0, ((0, 32), (2, 4)))
    prior_values = bell_draw(part_splits[15], (SEQS, PROP, HEADS * DV), 1.0, 6.0, ((0, 32), (2, 4)))
    prior_igate = bell_draw(part_splits[16], (SEQS, PROP, HEADS), 1.0, 4.0, ((0, 32), (2, 4)), jnp.float32)
    prior_fgate = jnp.clip(5.0 * jax.random.uniform(part_splits[17], (SEQS, PROP, HEADS), jnp.float32) ** block_scale(part_splits[17], (SEQS, PROP, HEADS), ((0, 32), (2, 4)), -0.2, 0.2), 0.0, 5.0)
    accepted = with_ends(jax.random.randint(part_splits[18], (SEQS,), 0, PROP + 1), jax.random.fold_in(part_splits[18], 1), 0, PROP).astype(jnp.int32)
    return {"tokens": tokens, "norm_gain": norm_gain, "w_query": w_query, "w_key": w_key, "w_value": w_value, "w_igate": w_igate, "w_fgate": w_fgate, "igate_bias": igate_bias, "fgate_bias": fgate_bias, "head_gain": head_gain, "w_out": w_out, "state_matrix": state_matrix, "state_norm": state_norm, "state_max": state_max, "prior_keys": prior_keys, "prior_values": prior_values, "prior_igate": prior_igate, "prior_fgate": prior_fgate, "accepted": accepted}


EPS = 1e-06

def heads_first(array, heads):
    seqs_n, props, width = array.shape
    return array.astype(jnp.float32).reshape(seqs_n, props, heads, width // heads).transpose(0, 2, 1, 3)

def fold_prior(matrix, normer, stabil, keys, values, in_pre, forget_pre, accepted):
    positions = jnp.arange(keys.shape[2], dtype=jnp.int32)
    active_mask = positions[None, None, :] < accepted[:, None, None]
    log_forget = jnp.where(active_mask, jax.nn.log_sigmoid(forget_pre), 0.0)
    in_gate = jnp.where(active_mask, in_pre, -1e+30)
    cum_forget = jnp.cumsum(log_forget, axis=-1)
    total_forget = cum_forget[..., -1]
    weight_log = total_forget[..., None] - cum_forget + in_gate
    new_stabil = jnp.maximum(total_forget + stabil, lax.optimization_barrier(jnp.max(weight_log, axis=-1)))
    carry_scale = jnp.exp(total_forget + stabil - new_stabil)
    weighted_keys = keys * jnp.exp(weight_log - new_stabil[..., None])[..., None]
    new_matrix = carry_scale[..., None, None] * matrix + jnp.einsum('bhtd,bhte->bhde', weighted_keys, values, precision=lax.Precision.HIGHEST)
    new_normer = carry_scale[..., None] * normer + lax.optimization_barrier(jnp.sum(weighted_keys, axis=2))
    return (new_matrix, new_normer, new_stabil)

def read_block(matrix, normer, stabil, query, keys, values, in_pre, forget_pre):
    props = query.shape[2]
    cum_forget = jnp.cumsum(jax.nn.log_sigmoid(forget_pre), axis=-1)
    causal = jnp.tril(jnp.ones((props, props), jnp.bool_))
    log_decay = jnp.where(causal, cum_forget[..., :, None] - cum_forget[..., None, :] + in_pre[..., None, :], -1e+30)
    inter = cum_forget + stabil[..., None]
    row_max = jnp.maximum(inter, lax.optimization_barrier(jnp.max(log_decay, axis=-1)))
    inter_scale = jnp.exp(inter - row_max)
    scores = jnp.einsum('bhtd,bhud->bhtu', query, keys, precision=lax.Precision.HIGHEST)
    scores = scores * jnp.exp(log_decay - row_max[..., None])
    numerator = inter_scale[..., None] * jnp.einsum('bhtd,bhde->bhte', query, matrix, precision=lax.Precision.HIGHEST)
    numerator = numerator + jnp.einsum('bhtu,bhue->bhte', scores, values, precision=lax.Precision.HIGHEST)
    denominator = inter_scale * jnp.einsum('bhtd,bhd->bht', query, normer, precision=lax.Precision.HIGHEST)
    denominator = denominator + lax.optimization_barrier(jnp.sum(scores, axis=-1))
    return numerator / jnp.maximum(jnp.abs(denominator), jnp.exp(-row_max))[..., None]

def head_norm(cell, head_gain):
    seqs_n, heads, props, width = cell.shape
    scaled = cell * lax.rsqrt(lax.optimization_barrier(jnp.mean(cell * cell, axis=-1, keepdims=True)) + EPS)
    scaled = scaled.transpose(0, 2, 1, 3).reshape(seqs_n * props, heads * width)
    return (scaled * head_gain.astype(jnp.float32)).astype(jnp.bfloat16)

def reference(tokens, norm_gain, w_query, w_key, w_value, w_igate, w_fgate, igate_bias, fgate_bias, head_gain, w_out, state_matrix, state_norm, state_max, prior_keys, prior_values, prior_igate, prior_fgate, accepted):
    inputs = tokens.astype(jnp.float32)
    normed = inputs * lax.rsqrt(lax.optimization_barrier(jnp.mean(inputs * inputs, axis=-1, keepdims=True)) + EPS)
    normed = (normed * norm_gain.astype(jnp.float32)).astype(jnp.bfloat16).reshape(SEQS * PROP, D)
    query = jnp.dot(normed, w_query, preferred_element_type=jnp.float32).astype(jnp.bfloat16)
    keys = jnp.dot(normed, w_key, preferred_element_type=jnp.float32).astype(jnp.bfloat16)
    values = jnp.dot(normed, w_value, preferred_element_type=jnp.float32).astype(jnp.bfloat16)
    in_pre = jnp.dot(normed, w_igate, preferred_element_type=jnp.float32) + igate_bias
    forget_pre = jnp.dot(normed, w_fgate, preferred_element_type=jnp.float32) + fgate_bias
    in_pre = in_pre.reshape(SEQS, PROP, HEADS).transpose(0, 2, 1)
    forget_pre = forget_pre.reshape(SEQS, PROP, HEADS).transpose(0, 2, 1)
    new_matrix, new_normer, new_stabil = fold_prior(state_matrix, state_norm, state_max, heads_first(prior_keys, HEADS) * DK ** (-0.5), heads_first(prior_values, HEADS), prior_igate.transpose(0, 2, 1), prior_fgate.transpose(0, 2, 1), accepted)
    cell = read_block(new_matrix, new_normer, new_stabil, heads_first(query.reshape(SEQS, PROP, -1), HEADS), heads_first(keys.reshape(SEQS, PROP, -1), HEADS) * DK ** (-0.5), heads_first(values.reshape(SEQS, PROP, -1), HEADS), in_pre, forget_pre)
    hidden = head_norm(cell, head_gain)
    mixed = jnp.dot(hidden, w_out, preferred_element_type=jnp.float32).reshape(SEQS, PROP, D)
    return (mixed, new_matrix, new_normer, new_stabil)
```

```python
import functools

import jax
import jax.numpy as jnp
from jax import lax
from jax.experimental import pallas as pl
from jax.experimental.pallas import tpu as pltpu
from jax.sharding import PartitionSpec as P

EPS = 1e-06
F32, BF16 = jnp.float32, jnp.bfloat16
MESH = pl.DeviceIdType.MESH
CORES = 2
HIGH = lax.Precision.HIGHEST
LAST = (((1,), (1,)), ((), ()))


def log_sigmoid(v):
    return jnp.minimum(v, 0.0) - jnp.log1p(jnp.exp(-jnp.abs(v)))


def kernel(
    dims,
    tok_h, ngain, wq_h, wk_h, wv_h, wig_h, wfg_h, igb, fgb, hgain, wo_h, st_h, sn_h, smax,
    pk_h, pv_h, pig, pfg, acc_n,
    mixed, nmat_h, nnorm, nmax,
    tok, xf, xb, wg, wo, acc, st, sb, pk, pv, sn, wig, wfg, kwb, vb, qb, qsb, gr, gc, ab, nrm,
    qall, sendq, hid, rsend, rrecv, own,
    loc, zs, zr, dsn, drc, xs, xr, qs_sem, qr_sem, rs_sem, rr_sem, ms,
):
    B, T, BP, NZ, TPN, HL, DK = dims
    R = T * BP
    g, kv, tp = lax.axis_index("grp"), lax.axis_index("kv"), lax.axis_index("tp")
    z, c = kv // CORES, lax.rem(kv, CORES)
    par = lax.rem(g, 2)
    mate = g + 1 - 2 * par
    KC = wq_h.shape[0]
    ZC = CORES * KC
    CW = wq_h.shape[1] // 2
    OC = wo_h.shape[1]
    HO = wo_h.shape[0] // 2
    LASTS = NZ // 2

    def zat(s, way):
        return lax.rem(z + NZ - s, NZ) if way == 0 else lax.rem(z + s, NZ)

    ring_to = (lax.rem(z + 1, NZ) * CORES + c, lax.rem(z + NZ - 1, NZ) * CORES + c)
    twin = z * CORES + 1 - c

    def slot(item, zz, cc):
        if item < 3:
            return wg.at[
                pl.ds(pl.multiple_of(zz * ZC + cc * KC, KC), KC), pl.ds(item * CW, CW)
            ]
        return wo.at[zz, pl.ds((item - 3) * HO, HO), pl.ds(pl.multiple_of(cc * OC, OC), OC)]

    def zcopy(item, way, s, shard):
        ref = slot(item, zat(shard, way), c)
        return pltpu.make_async_remote_copy(
            src_ref=ref, dst_ref=ref, send_sem=zs.at[item, way, s], recv_sem=zr.at[item, way, s],
            device_id={"kv": ring_to[way]}, device_id_type=MESH,
        )

    def dcopy(item, way, s, cc):
        ref = slot(item, zat(s, way), cc)
        return pltpu.make_async_remote_copy(
            src_ref=ref, dst_ref=ref, send_sem=dsn.at[item, way, s], recv_sem=drc.at[item, way, s],
            device_id={"kv": twin}, device_id_type=MESH,
        )

    def xcopy(zz, lo, hi):
        return pltpu.make_async_remote_copy(
            src_ref=xb.at[zz, pl.ds(lo, R), :], dst_ref=xb.at[zz, pl.ds(hi, R), :],
            send_sem=xs.at[zz], recv_sem=xr.at[zz],
            device_id={"grp": mate}, device_id_type=MESH,
        )

    def step(items, s, last_plus, last_minus, has_minus):
        for item in items:
            zcopy(item, 0, s - 1, s).wait_recv()
            if not last_plus:
                zcopy(item, 0, s, s).start()
            dcopy(item, 0, s, c).start()
            if has_minus:
                zcopy(item, 1, s - 1, s).wait_recv()
                if not last_minus:
                    zcopy(item, 1, s, s).start()
                dcopy(item, 1, s, c).start()

    def begin(items):
        for item in items:
            for way in (0, 1):
                zcopy(item, way, 0, 0).start()
            dcopy(item, 0, 0, c).start()

    def product(s, way):
        zz = zat(s, way)
        for item in range(3):
            dcopy(item, way, s, 1 - c).wait_recv()
        xcopy(zz, R, R).wait_recv()
        rows = pl.ds(pl.multiple_of(zz * ZC, ZC), ZC)
        return jnp.dot(xb[zz], wg[rows, :], preferred_element_type=F32)

    c0 = pl.multiple_of(par * CW, CW)
    mine = [
        pltpu.make_async_copy(src.at[:, pl.ds(c0, CW)], slot(i, z, c), loc.at[i])
        for i, src in enumerate((wq_h, wk_h, wv_h))
    ] + [
        pltpu.make_async_copy(wo_h.at[pl.ds(i * HO, HO), :], slot(3 + i, z, c), loc.at[3 + i])
        for i in range(2)
    ]
    loads = [
        pltpu.make_async_copy(src, dst, loc.at[5 + i])
        for i, (src, dst) in enumerate((
            (tok_h, tok), (wig_h, wig), (wfg_h, wfg), (pk_h, pk), (pv_h, pv), (sn_h, sn), (st_h, st),
        ))
    ]
    for cp in mine + loads:
        cp.start()
    barrier = pltpu.get_barrier_semaphore()
    for dev in (
        [{"kv": ring_to[0]}, {"kv": ring_to[1]}, {"kv": twin}, {"grp": mate}]
        + [{"tp": lax.rem(tp + d, TPN)} for d in range(1, TPN)]
    ):
        pl.semaphore_signal(barrier, inc=1, device_id=dev, device_id_type=MESH)
    for cp in mine:
        cp.wait()
    pl.semaphore_wait(barrier, 3 + TPN)
    begin((0, 1, 2))

    loads[0].wait()
    xf[...] = jnp.zeros_like(xf)

    def norm_rows(t, carry):
        v = tok[t].astype(F32)
        v = v * lax.rsqrt(jnp.mean(v * v, axis=-1, keepdims=True) + EPS) * ngain[...].astype(F32)
        xf[t, :B, :] = v
        return carry

    lax.fori_loop(0, T, norm_rows, 0)

    def cut_rows(i, carry):
        cols = pl.ds(pl.multiple_of(i * ZC, ZC), ZC)
        xb[i, :R, :] = xf[:, :, cols].reshape(R, ZC).astype(BF16)
        return carry

    lax.fori_loop(0, NZ, cut_rows, 0)
    for s in range(LASTS + 1):
        for way in (0, 1):
            if way == 0 or 0 < s < LASTS:
                xcopy(zat(s, way), 0, R).start()

    loads[1].wait()
    loads[2].wait()

    def gates(i, carry):
        a0, a1, b0, b1 = carry
        cols = pl.ds(pl.multiple_of(i * ZC, ZC), ZC)
        xi, wi, wf = xb[i, :R, :], wig[:, cols], wfg[:, cols]
        dot = functools.partial(lax.dot_general, dimension_numbers=LAST, preferred_element_type=F32)
        return a0 + dot(xi, wi), a1 + dot(xi, wf), b0 + dot(wi, xi), b1 + dot(wf, xi)

    zr_, zc_ = jnp.zeros((R, HL), F32), jnp.zeros((HL, R), F32)
    _, fr, ic, fc = lax.fori_loop(0, NZ, gates, (zr_, zr_, zc_, zc_))
    r0 = lax.broadcasted_iota(jnp.int32, (R, R), 0)
    r1 = lax.broadcasted_iota(jnp.int32, (R, R), 1)
    same = lax.rem(r0, BP) == lax.rem(r1, BP)
    upto = jnp.where(same & (r0 >= r1), 1.0, 0.0).astype(F32)
    cum_r = jnp.dot(
        upto, log_sigmoid(fr + fgb[...]), precision=HIGH, preferred_element_type=F32
    )
    lane_of = lambda ref: jnp.concatenate(
        [jnp.broadcast_to(ref[:, h : h + 1], (1, R)) for h in range(HL)], axis=0
    )
    cum_c = lax.dot_general(
        log_sigmoid(fc + lane_of(fgb)), upto, LAST, precision=HIGH, preferred_element_type=F32
    )
    gc[:HL, :] = ic + lane_of(igb) - cum_c

    lf, ig, run = [], [], None
    for t in range(T):
        live = t < acc_n[...]
        f = jnp.where(live, log_sigmoid(pfg[t]), 0.0)
        run = f if run is None else run + f
        lf.append(run)
        ig.append(jnp.where(live, pig[t], -1e30))
    wlog = [run - lf[t] + ig[t] for t in range(T)]
    top = functools.reduce(jnp.maximum, wlog)
    new_max = jnp.maximum(run + smax[...], top)
    nmax[...] = new_max
    eye = jnp.where(
        lax.broadcasted_iota(jnp.int32, (BP, B), 0) == lax.broadcasted_iota(jnp.int32, (BP, B), 1),
        1.0, 0.0,
    ).astype(F32)
    turn = lambda v: lax.dot_general(eye, v, LAST, precision=HIGH, preferred_element_type=F32)
    carry_r = turn(jnp.exp(run + smax[...] - new_max))
    max_r = turn(new_max)
    wts = [turn(jnp.exp(wlog[t] - new_max)) * (DK**-0.5) for t in range(T)]
    for h in range(HL):
        ab[h] = jnp.broadcast_to(carry_r[:, h : h + 1], (BP, DK))
        gr[h, 0] = jnp.broadcast_to(cum_r[:, h : h + 1], (R, DK))
        for t in range(T):
            gr[h, 1, t * BP : (t + 1) * BP] = jnp.broadcast_to(max_r[:, h : h + 1], (BP, DK))

    for cp in loads[3:6]:
        cp.wait()
    for ref in (kwb, vb, qb):
        ref[...] = jnp.zeros_like(ref)
    for h in range(HL):
        cols = slice(h * DK, (h + 1) * DK)
        total = None
        for t in range(T):
            kw = pk[t, :, cols].astype(F32) * wts[t][:B, h : h + 1]
            kwb[h, pl.ds(t, B, stride=8), :] = kw
            vb[h, pl.ds(t, B, stride=8), :] = pv[t, :, cols].astype(F32)
            total = kw if total is None else total + kw
        nrm[h, :B] = total
    for b in range(B):
        for h in range(HL):
            row = ab[h, b : b + 1] * sn[b, h : h + 1] + nrm[h, b : b + 1]
            nrm[h, b : b + 1] = row
            nnorm[b, h : h + 1] = row
    loads[6].wait()

    def fold(b):
        rows = pl.ds(pl.multiple_of(b * 8, 8), 8)
        for h in range(HL):
            outer = lax.dot_general(
                kwb[h, rows, :].astype(BF16), vb[h, rows, :].astype(BF16),
                (((0,), (0,)), ((), ())), preferred_element_type=F32,
            )
            s = st[b, h] * ab[h, pl.ds(b, 1), :] + outer
            st[b, h] = s
            sb[b, h] = s.astype(BF16)
        pltpu.make_async_copy(st.at[b], nmat_h.at[b], ms.at[b]).start()

    laps = LASTS - 3
    per = B // laps

    qkv = (0, 1, 2)
    step(qkv, 1, False, False, True)
    acc[...] = product(0, 0)
    for b in range(per * laps, B):
        fold(b)

    def ring(s, carry):
        step(qkv, s, False, False, True)
        acc[...] += product(s - 1, 0)
        acc[...] += product(s - 1, 1)
        for i in range(per):
            fold((s - 2) * per + i)
        return carry

    lax.fori_loop(2, LASTS - 1, ring, 0)
    step(qkv, LASTS - 1, False, True, True)
    begin((3, 4))
    acc[...] += product(LASTS - 2, 0)
    acc[...] += product(LASTS - 2, 1)
    step(qkv, LASTS, True, True, False)
    acc[...] += product(LASTS - 1, 0)
    acc[...] += product(LASTS - 1, 1)
    full = acc[...] + product(LASTS, 0)
    qcopies = []
    for j in range(3):
        cols = slice(j * CW, (j + 1) * CW)
        sendq[j] = full[R:, cols].astype(BF16)
        cp = pltpu.make_async_remote_copy(
            src_ref=sendq.at[j], dst_ref=qall.at[j, par], send_sem=qs_sem.at[j],
            recv_sem=qr_sem.at[j], device_id={"grp": mate}, device_id_type=MESH,
        )
        cp.start()
        qcopies.append(cp)
        qall[j, par] = full[:R, cols].astype(BF16)

    out_items = (3, 4)

    def out_step(s):
        step(out_items, s, s == LASTS, s >= LASTS - 1, s < LASTS)

    keep = same & (r0 >= r1) & (lax.rem(r1, BP) < B)

    def spread(half, i):
        h = half * 2 + i
        q = qall[0, half, :, i * DK : (i + 1) * DK].astype(F32)
        for t in range(T):
            qb[h, pl.ds(t, BP, stride=8), :] = q[t * BP : (t + 1) * BP]
        for b in range(B):
            rows = slice(b * 8, b * 8 + 8)
            qsb[h, rows, :] = jnp.dot(
                qb[h, rows, :].astype(BF16), sb[b, h], preferred_element_type=F32
            )

    def head(half, i):
        h = half * 2 + i
        cols = slice(i * DK, (i + 1) * DK)
        q, k, v = (qall[j, half, :, cols] for j in range(3))
        cum = gr[h, 0, :, :1]
        inter = cum + gr[h, 1, :, :1]
        decay = jnp.where(keep, cum + gc[pl.ds(h, 1), :], -1e30)
        top_r = jnp.maximum(inter, jnp.max(decay, axis=1, keepdims=True))
        scale = jnp.exp(inter - top_r)
        scores = lax.dot_general(q, k, LAST, preferred_element_type=F32) * (DK**-0.5)
        scores = scores * jnp.exp(decay - top_r)
        q32 = q.astype(F32)
        nh = nrm[h]
        read = jnp.concatenate(
            [qsb[h, pl.ds(t, BP, stride=8), :] for t in range(T)], axis=0
        )
        qn = jnp.concatenate(
            [
                jnp.sum(q32[t * BP : (t + 1) * BP] * nh, axis=1, keepdims=True)
                for t in range(T)
            ],
            axis=0,
        )
        num = scale * read + jnp.dot(scores.astype(BF16), v, preferred_element_type=F32)
        den = scale * qn + jnp.sum(scores, axis=1, keepdims=True)
        cell = num / jnp.maximum(jnp.abs(den), jnp.exp(-top_r))
        cell = cell * lax.rsqrt(jnp.mean(cell * cell, axis=1, keepdims=True) + EPS)
        hc = pl.ds(pl.multiple_of(h * DK, DK), DK)
        hid[:, hc] = (cell * hgain[:, hc].astype(F32)).astype(BF16)

    nrm[:, B:] = jnp.zeros((HL, BP - B, DK), F32)
    qsb[:, B * 8 :, :] = jnp.zeros((HL, (BP - B) * 8, DK), F32)
    spread(par, 0)
    out_step(1)
    spread(par, 1)
    out_step(2)
    head(par, 0)
    out_step(3)
    head(par, 1)
    for cp in qcopies:
        cp.wait_send()
    for j in range(3):
        pltpu.make_async_remote_copy(
            src_ref=sendq.at[j], dst_ref=qall.at[j, 1 - par], send_sem=qs_sem.at[j],
            recv_sem=qr_sem.at[j], device_id={"grp": mate}, device_id_type=MESH,
        ).wait_recv()
    out_step(4)
    spread(1 - par, 0)
    out_step(5)
    spread(1 - par, 1)
    out_step(6)
    head(1 - par, 0)
    out_step(7)
    head(1 - par, 1)
    out_step(8)
    for item in out_items:
        for s in range(LASTS + 1):
            dcopy(item, 0, s, 1 - c).wait_recv()
            if 0 < s < LASTS:
                dcopy(item, 1, s, 1 - c).wait_recv()

    per_tp = NZ // TPN
    NB = CORES * OC

    def block(target, i):
        return jnp.dot(hid[...], wo[target * per_tp + i], preferred_element_type=F32)

    sends = []
    for d in [TPN // 2] + [e for e in range(1, TPN) if e != TPN // 2]:
        target = lax.rem(tp + d, TPN)
        for i in range(per_tp):
            rsend[d - 1, :, i * NB : (i + 1) * NB] = block(target, i).astype(BF16)
        cp = pltpu.make_async_remote_copy(
            src_ref=rsend.at[d - 1], dst_ref=rrecv.at[d - 1], send_sem=rs_sem.at[d - 1],
            recv_sem=rr_sem.at[d - 1], device_id={"tp": target}, device_id_type=MESH,
        )
        cp.start()
        sends.append(cp)
    for i in range(per_tp):
        own[:, i * NB : (i + 1) * NB] = block(tp, i)

    def sent(s, carry):
        for item in range(5):
            for way in (0, 1):
                zcopy(item, way, s, s).wait_send()
                dcopy(item, way, s, c).wait_send()
        return carry

    for item in range(5):
        for way in (0, 1):
            zcopy(item, way, 0, 0).wait_send()
        dcopy(item, 0, 0, c).wait_send()
        zcopy(item, 0, LASTS - 1, LASTS - 1).wait_send()
        for way in (0, 1):
            dcopy(item, way, LASTS - 1, c).wait_send()
        dcopy(item, 0, LASTS, c).wait_send()
    lax.fori_loop(1, LASTS - 1, sent, 0)

    def x_sent(i, carry):
        xcopy(i, 0, R).wait_send()
        return carry

    lax.fori_loop(0, NZ, x_sent, 0)

    def m_sent(b, carry):
        pltpu.make_async_copy(st.at[b], nmat_h.at[b], ms.at[b]).wait()
        return carry

    lax.fori_loop(0, B, m_sent, 0)
    for cp in sends:
        cp.wait()
    for t in range(T):
        rows = slice(t * BP, (t + 1) * BP)
        total = own[rows]
        for d in range(TPN - 1):
            total = total + rrecv[d, rows].astype(F32)
        mixed[t] = total[:B]


def body(
    tokens, norm_gain, w_query, w_key, w_value, w_igate, w_fgate, igate_bias, fgate_bias,
    head_gain, w_out, state_matrix, state_norm, state_max, prior_keys, prior_values,
    prior_igate, prior_fgate, accepted,
):
    B, T, D = tokens.shape
    HL, DK = state_matrix.shape[1:3]
    NZ = lax.axis_size("kv") // CORES
    TPN = lax.axis_size("tp")
    BP = -(-B // 8) * 8
    R = T * BP
    W = w_query.shape[1]
    CW = W // 2
    KC = w_query.shape[0]
    ZC = KC * CORES
    OC = w_out.shape[1]
    OW = D // TPN
    VM = pl.BlockSpec(memory_space=pltpu.VMEM)
    HB = pl.BlockSpec(memory_space=pl.ANY)
    V, DMA = pltpu.VMEM, pltpu.SemaphoreType.DMA
    NS = NZ // 2 + 1
    outs = pl.pallas_call(
        functools.partial(kernel, (B, T, BP, NZ, TPN, HL, DK)),
        out_shape=(
            jax.ShapeDtypeStruct((T, B, OW), F32),
            jax.ShapeDtypeStruct(state_matrix.shape, F32),
            jax.ShapeDtypeStruct(state_norm.shape, F32),
            jax.ShapeDtypeStruct((HL, B), F32),
        ),
        in_specs=[HB, VM, HB, HB, HB, HB, HB, VM, VM, VM, HB, HB, HB, VM, HB, HB, VM, VM, VM],
        out_specs=(VM, HB, VM, VM),
        scratch_shapes=[
            V((T, B, D), BF16), V((T, BP, D), F32), V((NZ, 2 * R, ZC), BF16),
            V((D, 3 * CW), BF16), V((NZ, W, CORES * OC), BF16), V((2 * R, 3 * CW), F32),
            V(state_matrix.shape, F32), V(state_matrix.shape, BF16),
            V((T, B, W), BF16), V((T, B, W), BF16), V(state_norm.shape, F32),
            V((HL, D), BF16), V((HL, D), BF16),
            V((HL, BP * 8, DK), F32), V((HL, BP * 8, DK), F32),
            V((HL, BP * 8, DK), F32), V((HL, BP * 8, DK), F32),
            V((HL, 2, R, DK), F32), V((8, R), F32), V((HL, BP, DK), F32), V((HL, BP, DK), F32),
            V((3, 2, R, CW), BF16), V((3, R, CW), BF16), V((R, W), BF16),
            V((TPN - 1, R, OW), BF16), V((TPN - 1, R, OW), BF16), V((R, OW), F32),
            DMA((12,)), DMA((5, 2, NS)), DMA((5, 2, NS)), DMA((5, 2, NS)), DMA((5, 2, NS)),
            DMA((NZ,)), DMA((NZ,)), DMA((3,)), DMA((3,)), DMA((TPN - 1,)), DMA((TPN - 1,)),
            DMA((B,)),
        ],
        compiler_params=pltpu.CompilerParams(
            collective_id=0, has_side_effects=True, vmem_limit_bytes=60 * 1024 * 1024
        ),
        name="cell",
    )(
        tokens.transpose(1, 0, 2), norm_gain.reshape(1, -1), w_query, w_key, w_value,
        w_igate.T, w_fgate.T, igate_bias.reshape(1, -1), fgate_bias.reshape(1, -1),
        head_gain.reshape(1, -1), w_out, state_matrix, state_norm, state_max.T,
        prior_keys.transpose(1, 0, 2), prior_values.transpose(1, 0, 2),
        prior_igate.transpose(1, 2, 0), prior_fgate.transpose(1, 2, 0), accepted.reshape(1, -1),
    )
    mixed, new_matrix, new_norm, new_max = outs
    return mixed.transpose(1, 0, 2), new_matrix, new_norm, new_max.T


def solution(mesh):
    rows = ("grp", "kv")
    return jax.shard_map(
        body,
        mesh=mesh,
        in_specs=(
            P(rows, None, None), P(), P("kv", "tp"), P("kv", "tp"), P("kv", "tp"),
            P(None, "tp"), P(None, "tp"), P("tp"), P("tp"), P("tp"), P("tp", "kv"),
            P(rows, "tp", None, None), P(rows, "tp", None), P(rows, "tp"),
            P(rows, None, "tp"), P(rows, None, "tp"), P(rows, None, "tp"), P(rows, None, "tp"),
            P(rows),
        ),
        out_specs=(
            P(rows, None, "tp"), P(rows, "tp", None, None), P(rows, "tp", None), P(rows, "tp"),
        ),
        check_vma=False,
    )
```

```python
import functools

import jax
import jax.numpy as jnp
from jax import lax
from jax.experimental import pallas as pl
from jax.experimental.pallas import tpu as pltpu
from jax.sharding import PartitionSpec as P

EPS = 1e-06
F32, BF16 = jnp.float32, jnp.bfloat16
MESH = pl.DeviceIdType.MESH
CORES = 2
HIGH = lax.Precision.HIGHEST
LAST = (((1,), (1,)), ((), ()))


def log_sigmoid(v):
    return jnp.minimum(v, 0.0) - jnp.log1p(jnp.exp(-jnp.abs(v)))


def kernel(
    dims,
    tok_h, ngain, wq_h, wk_h, wv_h, wig_h, wfg_h, igb, fgb, hgain, wo_h, st_h, sn_h, smax,
    pk_h, pv_h, pig, pfg, acc_n,
    mixed, st, nnorm, nmax,
    tok, xf, xb, wg, wo, acc, sb, pk, pv, sn, wig, wfg, kwb, vb, qb, qsb, gr, gc, ab, nrm,
    g32, h32, qall, sendq, hid, rout, rin, part,
    loc, zs, zr, dsn, drc, drw, xs, xr, ys, yr, fs, fr_sem, qs_sem, qr_sem, rs_sem, rr_sem,
    left_in, twin_in, mate_in, tp_in,
):
    B, T, BP, NZ, TPN, HL, DK = dims
    R = T * BP
    g, kv, tp = lax.axis_index("grp"), lax.axis_index("kv"), lax.axis_index("tp")
    z, c = kv // CORES, lax.rem(kv, CORES)
    par = lax.rem(g, 2)
    mate = g + 1 - 2 * par
    KC = wq_h.shape[0]
    ZC = CORES * KC
    CW = wq_h.shape[1] // 2
    OC = wo_h.shape[1]
    HO = wo_h.shape[0] // 2
    N1 = (NZ - 1) * 3 // 5
    N0 = NZ - 1 - N1
    LATE = 4
    LAG = 2
    SLOTS = max(N1, N0 + LATE)
    corner = (z == 0) & (tp == 0)
    first = corner & (par == 0) & (c == 0)
    hold_twin = corner & (par == 0) & (c == 1)
    hold_mate = corner & (par == 1) & (c == 0)
    hold_sum = hold_twin | hold_mate
    hold_left = ((z == 0) & jnp.logical_not(first)) | (
        (z == 1) & (tp == 0) & (par == 0) & (c == 0)
    )
    prompt = jnp.where((tp == 0) & (par == 0), z - 1, z)

    def up(s):
        return lax.rem(z + s, NZ)

    def down(s):
        return lax.rem(z + NZ - s, NZ)

    def has1(k):
        return (k >= 1) & (k <= N1)

    def hop0(k):
        return jnp.where(k <= prompt, k, k - LATE)

    def has0(k):
        early = (k >= 1) & (k <= prompt) & (k <= N0)
        late = (k > prompt) & (k - LATE > prompt) & (k - LATE >= 1) & (k - LATE <= N0)
        return early | late

    ring_to = (up(1) * CORES + c, down(1) * CORES + c)
    twin = z * CORES + 1 - c

    def remote(src, dst, send, recv, dev):
        return pltpu.make_async_remote_copy(
            src_ref=src, dst_ref=dst, send_sem=send, recv_sem=recv,
            device_id=dev, device_id_type=MESH,
        )

    def slot(item, zz, cc, half):
        return wg.at[zz, item, cc] if item < 3 else wo.at[zz, cc, half]

    def zcopy(item, way, zz):
        ref = slot(item, zz, c, par)
        return remote(ref, ref, zs.at[item, way], zr.at[item, zz], {"kv": ring_to[way]})

    def dcopy(item, zz, cc):
        ref = slot(item, zz, cc, par)
        recv = drc.at[zz] if item < 3 else drw
        return remote(ref, ref, dsn.at[item], recv, {"kv": twin})

    def ycopy(zz, half):
        ref = wo.at[zz, c, half]
        return remote(ref, ref, ys, yr.at[zz], {"grp": mate})

    def fcopy(zz, cc):
        ref = wo.at[zz, cc, 1 - par]
        return remote(ref, ref, fs, fr_sem, {"kv": twin})

    def xcopy(zz, lo, hi):
        return remote(
            xb.at[zz, pl.ds(lo, R), :], xb.at[zz, pl.ds(hi, R), :], xs, xr.at[zz],
            {"grp": mate},
        )

    def onward(item, way, zz):
        zcopy(item, way, zz).start()

    def send_x():
        xcopy(z, 0, R).start()
        for s in range(1, N1 + 1):
            xcopy(up(s), 0, R).start()
            if s <= N0:
                xcopy(down(s), 0, R).start()

    def to_mate(item, zz):
        if item == 3:
            @pl.when(zz != z)
            def _():
                ycopy(zz, par).start()

    def to_twin(item, zz):
        dcopy(item, zz, c).start()
        if item == 3:
            @pl.when(zz == z)
            def _():
                fcopy(zz, c).start()

    def arrive(items, k, defer):
        low = hop0(k)
        zz1, zz0 = up(k), down(low)
        past = k > defer
        for item in items:
            @pl.when(has1(k))
            def _():
                zcopy(item, 1, zz1).wait_recv()

                @pl.when((k < N1) & (jnp.logical_not(hold_left) | past))
                def _():
                    onward(item, 1, zz1)

                @pl.when(jnp.logical_not(hold_twin) | past)
                def _():
                    to_twin(item, zz1)

                @pl.when(jnp.logical_not(hold_mate) | past)
                def _():
                    to_mate(item, zz1)

            @pl.when(has0(k))
            def _():
                zcopy(item, 0, zz0).wait_recv()

                @pl.when(low < N0)
                def _():
                    onward(item, 0, zz0)

                to_twin(item, zz0)
                to_mate(item, zz0)

        for hold, met, send in (
            (hold_left, lambda: pl.semaphore_wait(left_in, 1), lambda i, zz: onward(i, 1, zz)),
            (hold_twin, lambda: pl.semaphore_wait(twin_in, 1), to_twin),
            (hold_mate, lambda: pl.semaphore_wait(mate_in, 1), to_mate),
        ):
            @pl.when(hold & (k == defer))
            def _():
                if 3 not in items:
                    met()
                    if send is to_mate:
                        send_x()
                for s in range(defer + 1):
                    for item in items:
                        send(item, up(s))

    def begin(items):
        for item in items:
            onward(item, 0, z)

            @pl.when(jnp.logical_not(hold_left))
            def _():
                onward(item, 1, z)

            @pl.when(jnp.logical_not(hold_twin))
            def _():
                to_twin(item, z)

    def hand_over(k):
        @pl.when(has1(k))
        def _():
            ycopy(up(k), 1 - par).wait_recv()
            fcopy(up(k), c).start()

        @pl.when(has0(k))
        def _():
            ycopy(down(hop0(k)), 1 - par).wait_recv()
            fcopy(down(hop0(k)), c).start()

    def product(zz):
        both = wg.at[zz, :, 1 - c]
        remote(both, both, dsn.at[0], drc.at[zz], {"kv": twin}).wait_recv()
        xcopy(zz, R, R).wait_recv()
        x = xb[zz]
        return [
            jnp.dot(x, wg[zz, j].reshape(ZC, CW), preferred_element_type=F32) for j in range(3)
        ]

    def add_product(zz):
        for j, v in enumerate(product(zz)):
            acc[j] += v

    def products(k):
        @pl.when(has1(k))
        def _():
            add_product(up(k))

        @pl.when(has0(k))
        def _():
            add_product(down(hop0(k)))

    c0 = pl.multiple_of(par * CW, CW)
    mine = [
        pltpu.make_async_copy(src.at[:, pl.ds(c0, CW)], wg.at[z, i, c], loc.at[i])
        for i, src in enumerate((wq_h, wk_h, wv_h))
    ] + [
        pltpu.make_async_copy(wo_h.at[pl.ds(i * HO, HO), :], wo.at[z, c, i], loc.at[3 + i])
        for i in range(2)
    ]
    loads = [
        pltpu.make_async_copy(src, dst, loc.at[5 + i])
        for i, (src, dst) in enumerate((
            (tok_h, tok), (wig_h, wig), (wfg_h, wfg), (pk_h, pk), (pv_h, pv), (sn_h, sn), (st_h, st),
        ))
    ]
    barrier = pltpu.get_barrier_semaphore()

    def signal(sem, dev):
        pl.semaphore_signal(sem, inc=1, device_id=dev, device_id_type=MESH)

    right, left = lax.rem(tp + 1, TPN), lax.rem(tp + TPN - 1, TPN)
    tops, tops_l = tp < right, tp < left
    signal(barrier, {"kv": ring_to[1]})
    for cond, dev in (
        (c == 1, {"kv": twin}), (par == 1, {"grp": mate}),
        (jnp.logical_not(tops), {"tp": right}), (jnp.logical_not(tops_l), {"tp": left}),
    ):
        @pl.when(cond)
        def _():
            signal(barrier, dev)

    for cp in mine + loads:
        cp.start()
    for cp in mine:
        cp.wait()
    one = lambda cond: jnp.where(cond, 1, 0)
    pl.semaphore_wait(barrier, 1 + one(c == 0) + one(par == 0) + one(tops) + one(tops_l))
    signal(left_in, {"kv": ring_to[0]})
    for cond, sem, dev in (
        (c == 0, twin_in, {"kv": twin}), (par == 0, mate_in, {"grp": mate}),
        (tops, tp_in.at[0], {"tp": right}), (tops_l, tp_in.at[1], {"tp": left}),
    ):
        @pl.when(cond)
        def _():
            signal(sem, dev)

    @pl.when(jnp.logical_not(hold_left))
    def _():
        pl.semaphore_wait(left_in, 1)

    @pl.when((c == 1) & jnp.logical_not(hold_twin))
    def _():
        pl.semaphore_wait(twin_in, 1)

    @pl.when((par == 1) & jnp.logical_not(hold_mate))
    def _():
        pl.semaphore_wait(mate_in, 1)

    begin((0, 1, 2))

    loads[0].wait()
    g32[...] = ngain[...].astype(F32)
    h32[:HL] = hgain[...].astype(F32)
    xf[...] = jnp.zeros_like(xf)

    def norm_rows(t, carry):
        v = tok[t].astype(F32)
        xf[t, :B, :] = v * lax.rsqrt(jnp.mean(v * v, axis=-1, keepdims=True) + EPS)
        return carry

    lax.fori_loop(0, T, norm_rows, 0)
    LN = 128

    def cut_rows(i, carry):
        for j in range(ZC // LN):
            cols = pl.ds(pl.multiple_of(i * ZC + j * LN, LN), LN)
            v = xf[:, :, cols].reshape(R, LN) * g32[pl.ds(i * (ZC // LN) + j, 1), :]
            xb[i, :R, j * LN : (j + 1) * LN] = v.astype(BF16)
        return carry

    lax.fori_loop(0, NZ, cut_rows, 0)

    @pl.when(jnp.logical_not(hold_mate))
    def _():
        send_x()

    loads[1].wait()
    loads[2].wait()

    def gates(i, carry):
        a1, b0, b1 = carry
        cols = pl.ds(pl.multiple_of(i * ZC, ZC), ZC)
        xi, wi, wf = xb[i, :R, :], wig[:, cols], wfg[:, cols]
        dot = functools.partial(lax.dot_general, dimension_numbers=LAST, preferred_element_type=F32)
        return a1 + dot(xi, wf), b0 + dot(wi, xi), b1 + dot(wf, xi)

    zc_ = jnp.zeros((HL, R), F32)
    fr, ic, fc = lax.fori_loop(0, NZ, gates, (jnp.zeros((R, HL), F32), zc_, zc_))
    r0 = lax.broadcasted_iota(jnp.int32, (R, R), 0)
    r1 = lax.broadcasted_iota(jnp.int32, (R, R), 1)
    same = lax.rem(r0, BP) == lax.rem(r1, BP)
    upto = jnp.where(same & (r0 >= r1), 1.0, 0.0).astype(F32)
    cum_r = jnp.dot(
        upto, log_sigmoid(fr + fgb[...]), precision=HIGH, preferred_element_type=F32
    )
    lane_of = lambda ref: jnp.concatenate(
        [jnp.broadcast_to(ref[:, h : h + 1], (1, R)) for h in range(HL)], axis=0
    )
    cum_c = lax.dot_general(
        log_sigmoid(fc + lane_of(fgb)), upto, LAST, precision=HIGH, preferred_element_type=F32
    )
    gc[:HL, :] = ic + lane_of(igb) - cum_c

    lf, ig, run = [], [], None
    for t in range(T):
        live = t < acc_n[...]
        f = jnp.where(live, log_sigmoid(pfg[t]), 0.0)
        run = f if run is None else run + f
        lf.append(run)
        ig.append(jnp.where(live, pig[t], -1e30))
    wlog = [run - lf[t] + ig[t] for t in range(T)]
    top = functools.reduce(jnp.maximum, wlog)
    new_max = jnp.maximum(run + smax[...], top)
    nmax[...] = new_max
    eye = jnp.where(
        lax.broadcasted_iota(jnp.int32, (BP, B), 0) == lax.broadcasted_iota(jnp.int32, (BP, B), 1),
        1.0, 0.0,
    ).astype(F32)
    turn = lambda v: lax.dot_general(eye, v, LAST, precision=HIGH, preferred_element_type=F32)
    carry_r = turn(jnp.exp(run + smax[...] - new_max))
    max_r = turn(new_max)
    wts = [turn(jnp.exp(wlog[t] - new_max)) * (DK**-0.5) for t in range(T)]
    for h in range(HL):
        ab[h] = jnp.broadcast_to(carry_r[:, h : h + 1], (BP, DK))
        gr[h, 0] = jnp.broadcast_to(cum_r[:, h : h + 1], (R, DK))
        for t in range(T):
            gr[h, 1, t * BP : (t + 1) * BP] = jnp.broadcast_to(max_r[:, h : h + 1], (BP, DK))

    for cp in loads[3:6]:
        cp.wait()
    for ref in (kwb, vb, qb):
        ref[...] = jnp.zeros_like(ref)
    for h in range(HL):
        cols = slice(h * DK, (h + 1) * DK)
        total = None
        for t in range(T):
            kw = pk[t, :, cols].astype(F32) * wts[t][:B, h : h + 1]
            kwb[h, pl.ds(t, B, stride=8), :] = kw
            vb[h, pl.ds(t, B, stride=8), :] = pv[t, :, cols].astype(F32)
            total = kw if total is None else total + kw
        nrm[h, :B] = total
    for b in range(B):
        for h in range(HL):
            row = ab[h, b : b + 1] * sn[b, h : h + 1] + nrm[h, b : b + 1]
            nrm[h, b : b + 1] = row
            nnorm[b, h : h + 1] = row
    loads[6].wait()

    def fold(b):
        rows = pl.ds(pl.multiple_of(b * 8, 8), 8)
        for h in range(HL):
            outer = lax.dot_general(
                kwb[h, rows, :].astype(BF16), vb[h, rows, :].astype(BF16),
                (((0,), (0,)), ((), ())), preferred_element_type=F32,
            )
            s = st[b, h] * ab[h, pl.ds(b, 1), :] + outer
            st[b, h] = s
            sb[b, h] = s.astype(BF16)

    per = B // SLOTS
    for b in range(per * SLOTS, B):
        fold(b)

    acc[...] = jnp.zeros_like(acc)

    @pl.when(jnp.logical_not(hold_sum))
    def _():
        add_product(z)

    def ring(k, carry):
        arrive((0, 1, 2), k, LATE)

        @pl.when(k == LAG)
        def _():
            begin((3,))

        arrive((3,), k - LAG, LATE - LAG)

        @pl.when(jnp.logical_not(hold_sum) | (k > LATE + 1))
        def _():
            products(k - 1)

        @pl.when(hold_sum & (k == LATE + 1))
        def _():
            lax.fori_loop(0, LATE + 1, lambda s, c_: (add_product(up(s)), c_)[1], 0)

        for i in range(per):
            fold((k - 1) * per + i)
        return carry

    lax.fori_loop(1, SLOTS + 1, ring, 0)
    products(SLOTS)
    qcopies = []
    for j in range(3):
        sendq[j] = acc[j, R:].astype(BF16)
        cp = remote(
            sendq.at[j], qall.at[j, par], qs_sem.at[j], qr_sem.at[j], {"grp": mate}
        )
        cp.start()
        qcopies.append(cp)
        qall[j, par] = acc[j, :R].astype(BF16)

    def out_slot(k):
        arrive((3,), jnp.int32(k - LAG), LATE - LAG)

    keep = same & (r0 >= r1) & (lax.rem(r1, BP) < B)

    def spread(half, i):
        h = half * 2 + i
        q = qall[0, half, :, i * DK : (i + 1) * DK].astype(F32)
        for t in range(T):
            qb[h, pl.ds(t, BP, stride=8), :] = q[t * BP : (t + 1) * BP]
        for b in range(B):
            rows = slice(b * 8, b * 8 + 8)
            qsb[h, rows, :] = jnp.dot(
                qb[h, rows, :].astype(BF16), sb[b, h], preferred_element_type=F32
            )

    def head(half, i):
        h = half * 2 + i
        cols = slice(i * DK, (i + 1) * DK)
        q, k, v = (qall[j, half, :, cols] for j in range(3))
        cum = gr[h, 0, :, :1]
        inter = cum + gr[h, 1, :, :1]
        decay = jnp.where(keep, cum + gc[pl.ds(h, 1), :], -1e30)
        top_r = jnp.maximum(inter, jnp.max(decay, axis=1, keepdims=True))
        scale = jnp.exp(inter - top_r)
        scores = lax.dot_general(q, k, LAST, preferred_element_type=F32) * (DK**-0.5)
        scores = scores * jnp.exp(decay - top_r)
        q32 = q.astype(F32)
        nh = nrm[h]
        read = jnp.concatenate(
            [qsb[h, pl.ds(t, BP, stride=8), :] for t in range(T)], axis=0
        )
        qn = jnp.concatenate(
            [
                jnp.sum(q32[t * BP : (t + 1) * BP] * nh, axis=1, keepdims=True)
                for t in range(T)
            ],
            axis=0,
        )
        num = scale * read + jnp.dot(scores.astype(BF16), v, preferred_element_type=F32)
        den = scale * qn + jnp.sum(scores, axis=1, keepdims=True)
        cell = num / jnp.maximum(jnp.abs(den), jnp.exp(-top_r))
        cell = cell * lax.rsqrt(jnp.mean(cell * cell, axis=1, keepdims=True) + EPS)
        hc = pl.ds(pl.multiple_of(h * DK, DK), DK)
        hid[:, hc] = (cell * h32[pl.ds(h, 1), :]).astype(BF16)

    nrm[:, B:] = jnp.zeros((HL, BP - B, DK), F32)
    qsb[:, B * 8 :, :] = jnp.zeros((HL, (BP - B) * 8, DK), F32)
    def handed(lo, hi):
        def one_slot(k, carry):
            hand_over(k)
            return carry

        lax.fori_loop(lo, hi, one_slot, 0)

    steps = [
        lambda: (spread(par, 0), spread(par, 1)), lambda: head(par, 0), lambda: head(par, 1),
    ]
    for i in range(LAG):
        with jax.named_scope("outslot"):
            out_slot(SLOTS + 1 + i)
        if i < len(steps):
            steps[i]()
    for f in steps[LAG:]:
        f()
    handed(1, 5)
    for j, cp in enumerate(qcopies):
        cp.wait_send()
        remote(
            sendq.at[j], qall.at[j, 1 - par], qs_sem.at[j], qr_sem.at[j], {"grp": mate}
        ).wait_recv()
    spread(1 - par, 0)
    spread(1 - par, 1)
    head(1 - par, 0)
    head(1 - par, 1)
    with jax.named_scope("handed"):
        handed(5, SLOTS + 1)
    for half, sem in ((par, drw), (1 - par, fr_sem)):
        ref = wo.at[:, 1 - c, half]
        remote(ref, ref, fs, sem, {"kv": twin}).wait_recv()

    @pl.when(jnp.logical_not(tops))
    def _():
        pl.semaphore_wait(tp_in.at[1], 1)

    @pl.when(jnp.logical_not(tops_l))
    def _():
        pl.semaphore_wait(tp_in.at[0], 1)

    per_tp = NZ // TPN
    NB = CORES * OC
    HW = per_tp * NB // 2

    def block(target, i):
        zz = target * per_tp + i
        w = jnp.concatenate(
            [wo[zz, cc].reshape(2 * HO, OC) for cc in range(CORES)], axis=1
        )
        return jnp.dot(hid[...], w, preferred_element_type=F32)

    def chunk(target, half):
        n = per_tp // 2
        return jnp.concatenate([block(target, half * n + i) for i in range(n)], axis=1)

    def rcopy(i):
        return remote(
            rout.at[i], rin.at[i], rs_sem.at[i], rr_sem.at[i],
            {"tp": right if i % 2 == 0 else left},
        )

    far = lax.rem(tp + 2, TPN)
    for i, (target, half) in enumerate(((far, 0), (far, 1), (right, 1), (left, 0))):
        rout[i] = chunk(target, half).astype(BF16)
        rcopy(i).start()
    part[0] = chunk(right, 0)
    part[1] = chunk(left, 1)
    for i in range(2):
        rcopy(i).wait_recv()
        rout[4 + i] = (part[i] + rin[i].astype(F32)).astype(BF16)
        rcopy(4 + i).start()
    for i in range(2):
        part[i] = chunk(tp, i)

    def sent(ref, sem):
        remote(ref, ref, sem, drw, {"kv": twin}).wait_send()

    for item in range(4):
        kind = lambda n: wg.at[pl.ds(0, n), item, 0] if item < 3 else wo.at[pl.ds(0, n), 0, 0]
        sent(kind(N0), zs.at[item, 0])
        sent(kind(N1), zs.at[item, 1])
        sent(kind(NZ), dsn.at[item])
    sent(wo.at[pl.ds(0, NZ - 1), 0, 0], ys)
    sent(wo.at[pl.ds(0, NZ), 0, 0], fs)
    sent(xb.at[:, pl.ds(0, R), :], xs)
    for i in range(6):
        rcopy(i).wait_send()
        if i >= 2:
            rcopy(i).wait_recv()
    for t in range(T):
        rows = slice(t * BP, (t + 1) * BP)
        lo = part[0, rows] + rin[4, rows].astype(F32) + rin[3, rows].astype(F32)
        hi = part[1, rows] + rin[2, rows].astype(F32) + rin[5, rows].astype(F32)
        mixed[t, :, :HW] = lo[:B]
        mixed[t, :, HW:] = hi[:B]


def body(
    tokens, norm_gain, w_query, w_key, w_value, w_igate, w_fgate, igate_bias, fgate_bias,
    head_gain, w_out, state_matrix, state_norm, state_max, prior_keys, prior_values,
    prior_igate, prior_fgate, accepted,
):
    B, T, D = tokens.shape
    HL, DK = state_matrix.shape[1:3]
    NZ = lax.axis_size("kv") // CORES
    TPN = lax.axis_size("tp")
    BP = -(-B // 8) * 8
    R = T * BP
    W = w_query.shape[1]
    CW = W // 2
    KC = w_query.shape[0]
    ZC = KC * CORES
    OC = w_out.shape[1]
    OW = D // TPN
    VM = pl.BlockSpec(memory_space=pltpu.VMEM)
    HB = pl.BlockSpec(memory_space=pl.ANY)
    V, DMA, REG = pltpu.VMEM, pltpu.SemaphoreType.DMA, pltpu.SemaphoreType.REGULAR
    shapes = (
        jax.ShapeDtypeStruct((T, B, OW), F32),
        jax.ShapeDtypeStruct(state_matrix.shape, F32),
        jax.ShapeDtypeStruct(state_norm.shape, F32),
        jax.ShapeDtypeStruct((HL, B), F32),
    )
    outs = pl.pallas_call(
        functools.partial(kernel, (B, T, BP, NZ, TPN, HL, DK)),
        out_shape=tuple(V(a.shape, a.dtype) for a in shapes),
        in_specs=[HB, VM, HB, HB, HB, HB, HB, VM, VM, VM, HB, HB, HB, VM, HB, HB, VM, VM, VM],
        out_specs=(VM, VM, VM, VM),
        scratch_shapes=[
            V((T, B, D), BF16), V((T, BP, D), F32), V((NZ, 2 * R, ZC), BF16),
            V((NZ, 3, CORES, KC, CW), BF16), V((NZ, CORES, 2, W // 2, OC), BF16),
            V((3, 2 * R, CW), F32),
            V(state_matrix.shape, BF16),
            V((T, B, W), BF16), V((T, B, W), BF16), V(state_norm.shape, F32),
            V((HL, D), BF16), V((HL, D), BF16),
            V((HL, BP * 8, DK), F32), V((HL, BP * 8, DK), F32),
            V((HL, BP * 8, DK), F32), V((HL, BP * 8, DK), F32),
            V((HL, 2, R, DK), F32), V((8, R), F32), V((HL, BP, DK), F32), V((HL, BP, DK), F32),
            V((D // 128, 128), F32), V((8, DK), F32),
            V((3, 2, R, CW), BF16), V((3, R, CW), BF16), V((R, W), BF16),
            V((6, R, OW // 2), BF16), V((6, R, OW // 2), BF16), V((2, R, OW // 2), F32),
            DMA((12,)), DMA((4, 2)), DMA((4, NZ)), DMA((4,)), DMA((NZ,)), DMA,
            DMA, DMA((NZ,)), DMA, DMA((NZ,)), DMA, DMA,
            DMA((3,)), DMA((3,)), DMA((6,)), DMA((6,)),
            REG, REG, REG, pltpu.SemaphoreType.REGULAR((2,)),
        ],
        compiler_params=pltpu.CompilerParams(
            collective_id=0, has_side_effects=True, vmem_limit_bytes=56 * 1024 * 1024
        ),
        name="cell",
    )(
        tokens.transpose(1, 0, 2), norm_gain.reshape(-1, 128), w_query, w_key, w_value,
        w_igate.T, w_fgate.T, igate_bias.reshape(1, -1), fgate_bias.reshape(1, -1),
        head_gain.reshape(-1, DK), w_out, state_matrix, state_norm, state_max.T,
        prior_keys.transpose(1, 0, 2), prior_values.transpose(1, 0, 2),
        prior_igate.transpose(1, 2, 0), prior_fgate.transpose(1, 2, 0), accepted.reshape(1, -1),
    )
    mixed, new_matrix, new_norm, new_max = outs
    return mixed.transpose(1, 0, 2), new_matrix, new_norm, new_max.T


def solution(mesh):
    rows = ("grp", "kv")
    return jax.shard_map(
        body,
        mesh=mesh,
        in_specs=(
            P(rows, None, None), P(), P("kv", "tp"), P("kv", "tp"), P("kv", "tp"),
            P(None, "tp"), P(None, "tp"), P("tp"), P("tp"), P("tp"), P("tp", "kv"),
            P(rows, "tp", None, None), P(rows, "tp", None), P(rows, "tp"),
            P(rows, None, "tp"), P(rows, None, "tp"), P(rows, None, "tp"), P(rows, None, "tp"),
            P(rows),
        ),
        out_specs=(
            P(rows, None, "tp"), P(rows, "tp", None, None), P(rows, "tp", None), P(rows, "tp"),
        ),
        check_vma=False,
    )
```

```python
import functools

import jax
import jax.numpy as jnp
from jax import lax
from jax.experimental import pallas as pl
from jax.experimental.pallas import tpu as pltpu
from jax.sharding import PartitionSpec as P

EPS = 1e-06
F32, BF16 = jnp.float32, jnp.bfloat16
MESH = pl.DeviceIdType.MESH
CORES = 2
HIGH = lax.Precision.HIGHEST
LAST = (((1,), (1,)), ((), ()))


def log_sigmoid(v):
    return jnp.minimum(v, 0.0) - jnp.log1p(jnp.exp(-jnp.abs(v)))


def kernel(
    dims,
    tok_h, ngain, wq_h, wk_h, wv_h, wig_h, wfg_h, igb, fgb, hgain, wo_h, st_h, sn_h, smax,
    pk_h, pv_h, pig, pfg, acc_n,
    mixed, st, nnorm, nmax,
    tok, xf, xb, wg, wo, acc, sb, pk, pv, sn, wig, wfg, kwb, vb, qb, qsb, gr, gc, ab, nrm,
    g32, h32, qall, sendq, hid, rout, rin, part,
    loc, zs, zr, dsn, drc, drw, xs, xr, ys, yr, fs, fr_sem, qs_sem, qr_sem, rs_sem, rr_sem,
    left_in, twin_in, mate_in, tp_in,
):
    B, T, BP, NZ, TPN, HL, DK = dims
    R = T * BP
    g, kv, tp = lax.axis_index("grp"), lax.axis_index("kv"), lax.axis_index("tp")
    z, c = kv // CORES, lax.rem(kv, CORES)
    par = lax.rem(g, 2)
    mate = g + 1 - 2 * par
    KC = wq_h.shape[0]
    ZC = CORES * KC
    CW = wq_h.shape[1] // 2
    OC = wo_h.shape[1]
    HO = wo_h.shape[0] // 2
    N1 = (NZ - 1) * 3 // 5
    N0 = NZ - 1 - N1
    LATE = 3
    LAG = 2
    SLOTS = max(N1, N0 + LATE)
    corner = (z == 0) & (tp == 0)
    first = corner & (par == 0) & (c == 0)
    hold_twin = corner & (par == 0) & (c == 1)
    hold_mate = corner & (par == 1) & (c == 0)
    hold_sum = first | hold_twin | hold_mate
    hold_left = ((z == 0) & jnp.logical_not(first)) | (
        (z == 1) & (tp == 0) & (par == 0) & (c == 0)
    )
    prompt = jnp.where((tp == 0) & (par == 0), z - 1, z)

    def up(s):
        return lax.rem(z + s, NZ)

    def down(s):
        return lax.rem(z + NZ - s, NZ)

    def has1(k):
        return (k >= 1) & (k <= N1)

    def hop0(k):
        return jnp.where(k <= prompt, k, k - LATE)

    def has0(k):
        early = (k >= 1) & (k <= prompt) & (k <= N0)
        late = (k > prompt) & (k - LATE > prompt) & (k - LATE >= 1) & (k - LATE <= N0)
        return early | late

    ring_to = (up(1) * CORES + c, down(1) * CORES + c)
    twin = z * CORES + 1 - c

    def remote(src, dst, send, recv, dev):
        return pltpu.make_async_remote_copy(
            src_ref=src, dst_ref=dst, send_sem=send, recv_sem=recv,
            device_id=dev, device_id_type=MESH,
        )

    def slot(item, zz, cc, half):
        return wg.at[zz, item, cc] if item < 3 else wo.at[zz, cc, half]

    def zcopy(item, way, zz):
        ref = slot(item, zz, c, par)
        return remote(ref, ref, zs.at[item, way], zr.at[item, zz], {"kv": ring_to[way]})

    def dcopy(item, zz, cc):
        ref = slot(item, zz, cc, par)
        recv = drc.at[zz] if item < 3 else drw
        return remote(ref, ref, dsn.at[item], recv, {"kv": twin})

    def ycopy(zz, half):
        ref = wo.at[zz, c, half]
        return remote(ref, ref, ys, yr.at[zz], {"grp": mate})

    def fcopy(zz, cc):
        ref = wo.at[zz, cc, 1 - par]
        return remote(ref, ref, fs, fr_sem, {"kv": twin})

    def xcopy(zz, lo, hi):
        return remote(
            xb.at[zz, pl.ds(lo, R), :], xb.at[zz, pl.ds(hi, R), :], xs, xr.at[zz],
            {"grp": mate},
        )

    def onward(item, way, zz):
        zcopy(item, way, zz).start()

    def send_x():
        xcopy(z, 0, R).start()
        for s in range(1, N1 + 1):
            xcopy(up(s), 0, R).start()
            if s <= N0:
                xcopy(down(s), 0, R).start()

    def to_mate(item, zz):
        if item == 3:
            @pl.when(zz != z)
            def _():
                ycopy(zz, par).start()

    def to_twin(item, zz):
        dcopy(item, zz, c).start()
        if item == 3:
            @pl.when(zz == z)
            def _():
                fcopy(zz, c).start()

    def arrive(items, k, defer):
        low = hop0(k)
        zz1, zz0 = up(k), down(low)
        past = k > defer
        for item in items:
            @pl.when(has1(k))
            def _():
                zcopy(item, 1, zz1).wait_recv()

                @pl.when((k < N1) & (jnp.logical_not(hold_left) | past))
                def _():
                    onward(item, 1, zz1)

                @pl.when(jnp.logical_not(hold_twin) | past)
                def _():
                    to_twin(item, zz1)

                @pl.when(jnp.logical_not(hold_mate) | past)
                def _():
                    to_mate(item, zz1)

            @pl.when(has0(k))
            def _():
                zcopy(item, 0, zz0).wait_recv()

                @pl.when(low < N0)
                def _():
                    onward(item, 0, zz0)

                to_twin(item, zz0)
                to_mate(item, zz0)

        for hold, met, send in (
            (hold_left, lambda: pl.semaphore_wait(left_in, 1), lambda i, zz: onward(i, 1, zz)),
            (hold_twin, lambda: pl.semaphore_wait(twin_in, 1), to_twin),
            (hold_mate, lambda: pl.semaphore_wait(mate_in, 1), to_mate),
        ):
            @pl.when(hold & (k == defer))
            def _():
                if 3 not in items:
                    met()
                    if send is to_mate:
                        send_x()
                for s in range(defer + 1):
                    for item in items:
                        send(item, up(s))

    def begin(items):
        for item in items:
            onward(item, 0, z)

            @pl.when(jnp.logical_not(hold_left))
            def _():
                onward(item, 1, z)

            @pl.when(jnp.logical_not(hold_twin))
            def _():
                to_twin(item, z)

    def hand_over(k):
        @pl.when(has1(k))
        def _():
            ycopy(up(k), 1 - par).wait_recv()
            fcopy(up(k), c).start()

        @pl.when(has0(k))
        def _():
            ycopy(down(hop0(k)), 1 - par).wait_recv()
            fcopy(down(hop0(k)), c).start()

    def product(zz):
        both = wg.at[zz, :, 1 - c]
        remote(both, both, dsn.at[0], drc.at[zz], {"kv": twin}).wait_recv()
        xcopy(zz, R, R).wait_recv()
        x = xb[zz]
        return [
            jnp.dot(x, wg[zz, j].reshape(ZC, CW), preferred_element_type=F32) for j in range(3)
        ]

    def add_product(zz):
        for j, v in enumerate(product(zz)):
            acc[j] += v

    def products(k):
        @pl.when(has1(k))
        def _():
            add_product(up(k))

        @pl.when(has0(k))
        def _():
            add_product(down(hop0(k)))

    c0 = pl.multiple_of(par * CW, CW)
    mine = [
        pltpu.make_async_copy(src.at[:, pl.ds(c0, CW)], wg.at[z, i, c], loc.at[i])
        for i, src in enumerate((wq_h, wk_h, wv_h))
    ] + [
        pltpu.make_async_copy(wo_h.at[pl.ds(i * HO, HO), :], wo.at[z, c, i], loc.at[3 + i])
        for i in range(2)
    ]
    loads = [
        pltpu.make_async_copy(src, dst, loc.at[5 + i])
        for i, (src, dst) in enumerate((
            (tok_h, tok), (wig_h, wig), (wfg_h, wfg), (pk_h, pk), (pv_h, pv), (sn_h, sn), (st_h, st),
        ))
    ]
    barrier = pltpu.get_barrier_semaphore()

    def signal(sem, dev):
        pl.semaphore_signal(sem, inc=1, device_id=dev, device_id_type=MESH)

    right, left = lax.rem(tp + 1, TPN), lax.rem(tp + TPN - 1, TPN)
    tops, tops_l = tp < right, tp < left
    signal(barrier, {"kv": ring_to[1]})
    for cond, dev in (
        (c == 1, {"kv": twin}), (par == 1, {"grp": mate}),
        (jnp.logical_not(tops), {"tp": right}), (jnp.logical_not(tops_l), {"tp": left}),
    ):
        @pl.when(cond)
        def _():
            signal(barrier, dev)

    for cp in mine + loads:
        cp.start()
    for cp in mine:
        cp.wait()
    one = lambda cond: jnp.where(cond, 1, 0)
    pl.semaphore_wait(barrier, 1 + one(c == 0) + one(par == 0) + one(tops) + one(tops_l))
    signal(left_in, {"kv": ring_to[0]})
    for cond, sem, dev in (
        (c == 0, twin_in, {"kv": twin}), (par == 0, mate_in, {"grp": mate}),
        (tops, tp_in.at[0], {"tp": right}), (tops_l, tp_in.at[1], {"tp": left}),
    ):
        @pl.when(cond)
        def _():
            signal(sem, dev)

    @pl.when(jnp.logical_not(hold_left))
    def _():
        pl.semaphore_wait(left_in, 1)

    @pl.when((c == 1) & jnp.logical_not(hold_twin))
    def _():
        pl.semaphore_wait(twin_in, 1)

    @pl.when((par == 1) & jnp.logical_not(hold_mate))
    def _():
        pl.semaphore_wait(mate_in, 1)

    begin((0, 1, 2))

    loads[0].wait()
    g32[...] = ngain[...].astype(F32)
    h32[:HL] = hgain[...].astype(F32)
    xf[...] = jnp.zeros_like(xf)

    def norm_rows(t, carry):
        v = tok[t].astype(F32)
        xf[t, :B, :] = v * lax.rsqrt(jnp.mean(v * v, axis=-1, keepdims=True) + EPS)
        return carry

    lax.fori_loop(0, T, norm_rows, 0)
    LN = 128

    def cut_rows(i, carry):
        for j in range(ZC // LN):
            cols = pl.ds(pl.multiple_of(i * ZC + j * LN, LN), LN)
            v = xf[:, :, cols].reshape(R, LN) * g32[pl.ds(i * (ZC // LN) + j, 1), :]
            xb[i, :R, j * LN : (j + 1) * LN] = v.astype(BF16)
        return carry

    lax.fori_loop(0, NZ, cut_rows, 0)

    @pl.when(jnp.logical_not(hold_mate))
    def _():
        send_x()

    loads[1].wait()
    loads[2].wait()

    def gates(i, carry):
        a1, b0, b1 = carry
        cols = pl.ds(pl.multiple_of(i * ZC, ZC), ZC)
        xi, wi, wf = xb[i, :R, :], wig[:, cols], wfg[:, cols]
        dot = functools.partial(lax.dot_general, dimension_numbers=LAST, preferred_element_type=F32)
        return a1 + dot(xi, wf), b0 + dot(wi, xi), b1 + dot(wf, xi)

    zc_ = jnp.zeros((HL, R), F32)
    fr, ic, fc = lax.fori_loop(0, NZ, gates, (jnp.zeros((R, HL), F32), zc_, zc_))
    r0 = lax.broadcasted_iota(jnp.int32, (R, R), 0)
    r1 = lax.broadcasted_iota(jnp.int32, (R, R), 1)
    same = lax.rem(r0, BP) == lax.rem(r1, BP)
    upto = jnp.where(same & (r0 >= r1), 1.0, 0.0).astype(F32)
    cum_r = jnp.dot(
        upto, log_sigmoid(fr + fgb[...]), precision=HIGH, preferred_element_type=F32
    )
    lane_of = lambda ref: jnp.concatenate(
        [jnp.broadcast_to(ref[:, h : h + 1], (1, R)) for h in range(HL)], axis=0
    )
    cum_c = lax.dot_general(
        log_sigmoid(fc + lane_of(fgb)), upto, LAST, precision=HIGH, preferred_element_type=F32
    )
    gc[:HL, :] = ic + lane_of(igb) - cum_c

    lf, ig, run = [], [], None
    for t in range(T):
        live = t < acc_n[...]
        f = jnp.where(live, log_sigmoid(pfg[t]), 0.0)
        run = f if run is None else run + f
        lf.append(run)
        ig.append(jnp.where(live, pig[t], -1e30))
    wlog = [run - lf[t] + ig[t] for t in range(T)]
    top = functools.reduce(jnp.maximum, wlog)
    new_max = jnp.maximum(run + smax[...], top)
    nmax[...] = new_max
    eye = jnp.where(
        lax.broadcasted_iota(jnp.int32, (BP, B), 0) == lax.broadcasted_iota(jnp.int32, (BP, B), 1),
        1.0, 0.0,
    ).astype(F32)
    turn = lambda v: lax.dot_general(eye, v, LAST, precision=HIGH, preferred_element_type=F32)
    carry_r = turn(jnp.exp(run + smax[...] - new_max))
    max_r = turn(new_max)
    wts = [turn(jnp.exp(wlog[t] - new_max)) * (DK**-0.5) for t in range(T)]
    for h in range(HL):
        ab[h] = jnp.broadcast_to(carry_r[:, h : h + 1], (BP, DK))
        gr[h, 0] = jnp.broadcast_to(cum_r[:, h : h + 1], (R, DK))
        for t in range(T):
            gr[h, 1, t * BP : (t + 1) * BP] = jnp.broadcast_to(max_r[:, h : h + 1], (BP, DK))

    for cp in loads[3:6]:
        cp.wait()
    for ref in (kwb, vb, qb):
        ref[...] = jnp.zeros_like(ref)
    for h in range(HL):
        cols = slice(h * DK, (h + 1) * DK)
        total = None
        for t in range(T):
            kw = pk[t, :, cols].astype(F32) * wts[t][:B, h : h + 1]
            kwb[h, pl.ds(t, B, stride=8), :] = kw
            vb[h, pl.ds(t, B, stride=8), :] = pv[t, :, cols].astype(F32)
            total = kw if total is None else total + kw
        nrm[h, :B] = total
    for b in range(B):
        for h in range(HL):
            row = ab[h, b : b + 1] * sn[b, h : h + 1] + nrm[h, b : b + 1]
            nrm[h, b : b + 1] = row
            nnorm[b, h : h + 1] = row
    loads[6].wait()

    def fold(b):
        rows = pl.ds(pl.multiple_of(b * 8, 8), 8)
        for h in range(HL):
            outer = lax.dot_general(
                kwb[h, rows, :].astype(BF16), vb[h, rows, :].astype(BF16),
                (((0,), (0,)), ((), ())), preferred_element_type=F32,
            )
            s = st[b, h] * ab[h, pl.ds(b, 1), :] + outer
            st[b, h] = s
            sb[b, h] = s.astype(BF16)

    per = B // SLOTS
    for b in range(per * SLOTS, B):
        fold(b)

    acc[...] = jnp.zeros_like(acc)

    @pl.when(jnp.logical_not(hold_sum))
    def _():
        add_product(z)

    def ring(k, carry):
        arrive((0, 1, 2), k, LATE)

        @pl.when(k == LAG)
        def _():
            begin((3,))

        arrive((3,), k - LAG, LATE - LAG)

        @pl.when(jnp.logical_not(hold_sum) | (k > LATE + 1))
        def _():
            products(k - 1)

        @pl.when(hold_sum & (k == LATE + 1))
        def _():
            lax.fori_loop(0, LATE + 1, lambda s, c_: (add_product(up(s)), c_)[1], 0)

        for i in range(per):
            fold((k - 1) * per + i)
        return carry

    lax.fori_loop(1, SLOTS + 1, ring, 0)
    products(SLOTS)

    def qcopy(j, i, half):
        cols = pl.ds(i * DK, DK)
        return remote(
            sendq.at[j, :, cols], qall.at[j, half, :, cols], qs_sem.at[j, i], qr_sem.at[j, i],
            {"grp": mate},
        )

    for i in range(2):
        for j in range(3):
            cols = slice(i * DK, (i + 1) * DK)
            sendq[j, :, cols] = acc[j, R:, cols].astype(BF16)
            qcopy(j, i, par).start()
    for j in range(3):
        qall[j, par] = acc[j, :R].astype(BF16)

    def out_slot(k):
        arrive((3,), jnp.int32(k - LAG), LATE - LAG)

    keep = same & (r0 >= r1) & (lax.rem(r1, BP) < B)

    def spread(half, i):
        h = half * 2 + i
        q = qall[0, half, :, i * DK : (i + 1) * DK].astype(F32)
        for t in range(T):
            qb[h, pl.ds(t, BP, stride=8), :] = q[t * BP : (t + 1) * BP]
        for b in range(B):
            rows = slice(b * 8, b * 8 + 8)
            qsb[h, rows, :] = jnp.dot(
                qb[h, rows, :].astype(BF16), sb[b, h], preferred_element_type=F32
            )

    def head(half, i):
        h = half * 2 + i
        cols = slice(i * DK, (i + 1) * DK)
        q, k, v = (qall[j, half, :, cols] for j in range(3))
        cum = gr[h, 0, :, :1]
        inter = cum + gr[h, 1, :, :1]
        decay = jnp.where(keep, cum + gc[pl.ds(h, 1), :], -1e30)
        top_r = jnp.maximum(inter, jnp.max(decay, axis=1, keepdims=True))
        scale = jnp.exp(inter - top_r)
        scores = lax.dot_general(q, k, LAST, preferred_element_type=F32) * (DK**-0.5)
        scores = scores * jnp.exp(decay - top_r)
        q32 = q.astype(F32)
        nh = nrm[h]
        read = jnp.concatenate(
            [qsb[h, pl.ds(t, BP, stride=8), :] for t in range(T)], axis=0
        )
        qn = jnp.concatenate(
            [
                jnp.sum(q32[t * BP : (t + 1) * BP] * nh, axis=1, keepdims=True)
                for t in range(T)
            ],
            axis=0,
        )
        num = scale * read + jnp.dot(scores.astype(BF16), v, preferred_element_type=F32)
        den = scale * qn + jnp.sum(scores, axis=1, keepdims=True)
        cell = num / jnp.maximum(jnp.abs(den), jnp.exp(-top_r))
        cell = cell * lax.rsqrt(jnp.mean(cell * cell, axis=1, keepdims=True) + EPS)
        hc = pl.ds(pl.multiple_of(h * DK, DK), DK)
        hid[:, hc] = (cell * h32[pl.ds(h, 1), :]).astype(BF16)

    nrm[:, B:] = jnp.zeros((HL, BP - B, DK), F32)
    qsb[:, B * 8 :, :] = jnp.zeros((HL, (BP - B) * 8, DK), F32)
    def handed(lo, hi):
        def one_slot(k, carry):
            hand_over(k)
            return carry

        lax.fori_loop(lo, hi, one_slot, 0)

    steps = [
        lambda: (spread(par, 0), spread(par, 1)), lambda: head(par, 0), lambda: head(par, 1),
    ]
    for i in range(LAG):
        with jax.named_scope("outslot"):
            out_slot(SLOTS + 1 + i)
        if i < len(steps):
            steps[i]()
    for f in steps[LAG:]:
        f()
    handed(1, 5)
    for i in range(2):
        with jax.named_scope("qwait"):
            for j in range(3):
                qcopy(j, i, par).wait_send()
                qcopy(j, i, 1 - par).wait_recv()
        spread(1 - par, i)
        head(1 - par, i)
    with jax.named_scope("handed"):
        handed(5, SLOTS + 1)
    for half, sem in ((par, drw), (1 - par, fr_sem)):
        ref = wo.at[:, 1 - c, half]
        remote(ref, ref, fs, sem, {"kv": twin}).wait_recv()

    @pl.when(jnp.logical_not(tops))
    def _():
        pl.semaphore_wait(tp_in.at[1], 1)

    @pl.when(jnp.logical_not(tops_l))
    def _():
        pl.semaphore_wait(tp_in.at[0], 1)

    per_tp = NZ // TPN
    NB = CORES * OC
    HW = per_tp * NB // 2

    def block(target, i):
        zz = target * per_tp + i
        w = jnp.concatenate(
            [wo[zz, cc].reshape(2 * HO, OC) for cc in range(CORES)], axis=1
        )
        return jnp.dot(hid[...], w, preferred_element_type=F32)

    def chunk(target, half):
        n = per_tp // 2
        return jnp.concatenate([block(target, half * n + i) for i in range(n)], axis=1)

    def rcopy(i):
        return remote(
            rout.at[i], rin.at[i], rs_sem.at[i], rr_sem.at[i],
            {"tp": right if i % 2 == 0 else left},
        )

    far = lax.rem(tp + 2, TPN)
    for i, (target, half) in enumerate(((far, 0), (far, 1), (right, 1), (left, 0))):
        rout[i] = chunk(target, half).astype(BF16)
        rcopy(i).start()
    part[0] = chunk(right, 0)
    part[1] = chunk(left, 1)
    for i in range(2):
        rcopy(i).wait_recv()
        rout[4 + i] = (part[i] + rin[i].astype(F32)).astype(BF16)
        rcopy(4 + i).start()
    for i in range(2):
        part[i] = chunk(tp, i)

    def sent(ref, sem):
        remote(ref, ref, sem, drw, {"kv": twin}).wait_send()

    for item in range(4):
        kind = lambda n: wg.at[pl.ds(0, n), item, 0] if item < 3 else wo.at[pl.ds(0, n), 0, 0]
        sent(kind(N0), zs.at[item, 0])
        sent(kind(N1), zs.at[item, 1])
        sent(kind(NZ), dsn.at[item])
    sent(wo.at[pl.ds(0, NZ - 1), 0, 0], ys)
    sent(wo.at[pl.ds(0, NZ), 0, 0], fs)
    sent(xb.at[:, pl.ds(0, R), :], xs)
    for i in range(6):
        rcopy(i).wait_send()
        if i >= 2:
            rcopy(i).wait_recv()
    for t in range(T):
        rows = slice(t * BP, (t + 1) * BP)
        lo = part[0, rows] + rin[4, rows].astype(F32) + rin[3, rows].astype(F32)
        hi = part[1, rows] + rin[2, rows].astype(F32) + rin[5, rows].astype(F32)
        mixed[t, :, :HW] = lo[:B]
        mixed[t, :, HW:] = hi[:B]


def body(
    tokens, norm_gain, w_query, w_key, w_value, w_igate, w_fgate, igate_bias, fgate_bias,
    head_gain, w_out, state_matrix, state_norm, state_max, prior_keys, prior_values,
    prior_igate, prior_fgate, accepted,
):
    B, T, D = tokens.shape
    HL, DK = state_matrix.shape[1:3]
    NZ = lax.axis_size("kv") // CORES
    TPN = lax.axis_size("tp")
    BP = -(-B // 8) * 8
    R = T * BP
    W = w_query.shape[1]
    CW = W // 2
    KC = w_query.shape[0]
    ZC = KC * CORES
    OC = w_out.shape[1]
    OW = D // TPN
    VM = pl.BlockSpec(memory_space=pltpu.VMEM)
    HB = pl.BlockSpec(memory_space=pl.ANY)
    V, DMA, REG = pltpu.VMEM, pltpu.SemaphoreType.DMA, pltpu.SemaphoreType.REGULAR
    shapes = (
        jax.ShapeDtypeStruct((T, B, OW), F32),
        jax.ShapeDtypeStruct(state_matrix.shape, F32),
        jax.ShapeDtypeStruct(state_norm.shape, F32),
        jax.ShapeDtypeStruct((HL, B), F32),
    )
    outs = pl.pallas_call(
        functools.partial(kernel, (B, T, BP, NZ, TPN, HL, DK)),
        out_shape=tuple(V(a.shape, a.dtype) for a in shapes),
        in_specs=[HB, VM, HB, HB, HB, HB, HB, VM, VM, VM, HB, HB, HB, VM, HB, HB, VM, VM, VM],
        out_specs=(VM, VM, VM, VM),
        scratch_shapes=[
            V((T, B, D), BF16), V((T, BP, D), F32), V((NZ, 2 * R, ZC), BF16),
            V((NZ, 3, CORES, KC, CW), BF16), V((NZ, CORES, 2, W // 2, OC), BF16),
            V((3, 2 * R, CW), F32),
            V(state_matrix.shape, BF16),
            V((T, B, W), BF16), V((T, B, W), BF16), V(state_norm.shape, F32),
            V((HL, D), BF16), V((HL, D), BF16),
            V((HL, BP * 8, DK), F32), V((HL, BP * 8, DK), F32),
            V((HL, BP * 8, DK), F32), V((HL, BP * 8, DK), F32),
            V((HL, 2, R, DK), F32), V((8, R), F32), V((HL, BP, DK), F32), V((HL, BP, DK), F32),
            V((D // 128, 128), F32), V((8, DK), F32),
            V((3, 2, R, CW), BF16), V((3, R, CW), BF16), V((R, W), BF16),
            V((6, R, OW // 2), BF16), V((6, R, OW // 2), BF16), V((2, R, OW // 2), F32),
            DMA((12,)), DMA((4, 2)), DMA((4, NZ)), DMA((4,)), DMA((NZ,)), DMA,
            DMA, DMA((NZ,)), DMA, DMA((NZ,)), DMA, DMA,
            DMA((3, 2)), DMA((3, 2)), DMA((6,)), DMA((6,)),
            REG, REG, REG, pltpu.SemaphoreType.REGULAR((2,)),
        ],
        compiler_params=pltpu.CompilerParams(
            collective_id=0, has_side_effects=True, vmem_limit_bytes=56 * 1024 * 1024
        ),
        name="cell",
    )(
        tokens.transpose(1, 0, 2), norm_gain.reshape(-1, 128), w_query, w_key, w_value,
        w_igate.T, w_fgate.T, igate_bias.reshape(1, -1), fgate_bias.reshape(1, -1),
        head_gain.reshape(-1, DK), w_out, state_matrix, state_norm, state_max.T,
        prior_keys.transpose(1, 0, 2), prior_values.transpose(1, 0, 2),
        prior_igate.transpose(1, 2, 0), prior_fgate.transpose(1, 2, 0), accepted.reshape(1, -1),
    )
    mixed, new_matrix, new_norm, new_max = outs
    return mixed.transpose(1, 0, 2), new_matrix, new_norm, new_max.T


def solution(mesh):
    rows = ("grp", "kv")
    return jax.shard_map(
        body,
        mesh=mesh,
        in_specs=(
            P(rows, None, None), P(), P("kv", "tp"), P("kv", "tp"), P("kv", "tp"),
            P(None, "tp"), P(None, "tp"), P("tp"), P("tp"), P("tp"), P("tp", "kv"),
            P(rows, "tp", None, None), P(rows, "tp", None), P(rows, "tp"),
            P(rows, None, "tp"), P(rows, None, "tp"), P(rows, None, "tp"), P(rows, None, "tp"),
            P(rows),
        ),
        out_specs=(
            P(rows, None, "tp"), P(rows, "tp", None, None), P(rows, "tp", None), P(rows, "tp"),
        ),
        check_vma=False,
    )
```

```python
import functools

import jax
import jax.numpy as jnp
from jax import lax
from jax.experimental import pallas as pl
from jax.experimental.pallas import tpu as pltpu
from jax.sharding import PartitionSpec as P

EPS = 1e-06
F32, BF16 = jnp.float32, jnp.bfloat16
MESH = pl.DeviceIdType.MESH
CORES = 2
HIGH = lax.Precision.HIGHEST
LAST = (((1,), (1,)), ((), ()))


def log_sigmoid(v):
    return jnp.minimum(v, 0.0) - jnp.log1p(jnp.exp(-jnp.abs(v)))


def kernel(
    dims,
    tok_h, ngain, wq_h, wk_h, wv_h, wig_h, wfg_h, igb, fgb, hgain, wo_h, st_h, sn_h, smax,
    pk_h, pv_h, pig, pfg, acc_n,
    mixed, st, nnorm, nmax,
    tok, xf, xb, wg, wo, acc, sb, pk, pv, sn, wig, wfg, kwb, vb, qb, qsb, gr, gc, ab, nrm,
    g32, h32, qall, sendq, hid, rout, rin, part,
    loc, zs, zr, dsn, drc, drw, xs, xr, ys, yr, fs, fr_sem, qs_sem, qr_sem, rs_sem, rr_sem,
    left_in, twin_in, mate_in, tp_in,
):
    B, T, BP, NZ, TPN, HL, DK = dims
    R = T * BP
    g, kv, tp = lax.axis_index("grp"), lax.axis_index("kv"), lax.axis_index("tp")
    z, c = kv // CORES, lax.rem(kv, CORES)
    par = lax.rem(g, 2)
    mate = g + 1 - 2 * par
    KC = wq_h.shape[0]
    ZC = CORES * KC
    CW = wq_h.shape[1] // 2
    OC = wo_h.shape[1]
    HO = wo_h.shape[0] // 2
    N1 = (NZ - 1) * 3 // 5
    N0 = NZ - 1 - N1
    LATE = 3
    LAG = 2
    SLOTS = max(N1, N0 + LATE)
    corner = (z == 0) & (tp == 0)
    first = corner & (par == 0) & (c == 0)
    hold_twin = corner & (par == 0) & (c == 1)
    hold_mate = corner & (par == 1) & (c == 0)
    hold_sum = first | hold_twin | hold_mate
    hold_left = ((z == 0) & jnp.logical_not(first)) | (
        (z == 1) & (tp == 0) & (par == 0) & (c == 0)
    )
    prompt = jnp.where((tp == 0) & (par == 0), z - 1, z)

    def up(s):
        return lax.rem(z + s, NZ)

    def down(s):
        return lax.rem(z + NZ - s, NZ)

    def has1(k):
        return (k >= 1) & (k <= N1)

    def hop0(k):
        return jnp.where(k <= prompt, k, k - LATE)

    def has0(k):
        early = (k >= 1) & (k <= prompt) & (k <= N0)
        late = (k > prompt) & (k - LATE > prompt) & (k - LATE >= 1) & (k - LATE <= N0)
        return early | late

    ring_to = (up(1) * CORES + c, down(1) * CORES + c)
    twin = z * CORES + 1 - c

    def remote(src, dst, send, recv, dev):
        return pltpu.make_async_remote_copy(
            src_ref=src, dst_ref=dst, send_sem=send, recv_sem=recv,
            device_id=dev, device_id_type=MESH,
        )

    def slot(item, zz, cc, half):
        return wg.at[zz, item, cc] if item < 3 else wo.at[zz, cc, half]

    def zcopy(item, way, zz):
        ref = slot(item, zz, c, par)
        return remote(ref, ref, zs.at[item, way], zr.at[item, zz], {"kv": ring_to[way]})

    def dcopy(item, zz, cc):
        ref = slot(item, zz, cc, par)
        recv = drc.at[zz] if item < 3 else drw
        return remote(ref, ref, dsn.at[item], recv, {"kv": twin})

    def ycopy(zz, half):
        ref = wo.at[zz, c, half]
        return remote(ref, ref, ys, yr.at[zz], {"grp": mate})

    def fcopy(zz, cc):
        ref = wo.at[zz, cc, 1 - par]
        return remote(ref, ref, fs, fr_sem, {"kv": twin})

    def xcopy(zz, lo, hi):
        return remote(
            xb.at[zz, pl.ds(lo, R), :], xb.at[zz, pl.ds(hi, R), :], xs, xr.at[zz],
            {"grp": mate},
        )

    def onward(item, way, zz):
        zcopy(item, way, zz).start()

    def send_x():
        xcopy(z, 0, R).start()
        for s in range(1, N1 + 1):
            xcopy(up(s), 0, R).start()
            if s <= N0:
                xcopy(down(s), 0, R).start()

    def to_mate(item, zz):
        if item == 3:
            @pl.when(zz != z)
            def _():
                ycopy(zz, par).start()

    def to_twin(item, zz):
        dcopy(item, zz, c).start()
        if item == 3:
            @pl.when(zz == z)
            def _():
                fcopy(zz, c).start()

    def arrive(items, k, defer):
        low = hop0(k)
        zz1, zz0 = up(k), down(low)
        past = k > defer
        for item in items:
            @pl.when(has1(k))
            def _():
                zcopy(item, 1, zz1).wait_recv()

                @pl.when((k < N1) & (jnp.logical_not(hold_left) | past))
                def _():
                    onward(item, 1, zz1)

                @pl.when(jnp.logical_not(hold_twin) | past)
                def _():
                    to_twin(item, zz1)

                @pl.when(jnp.logical_not(hold_mate) | past)
                def _():
                    to_mate(item, zz1)

            @pl.when(has0(k))
            def _():
                zcopy(item, 0, zz0).wait_recv()

                @pl.when(low < N0)
                def _():
                    onward(item, 0, zz0)

                to_twin(item, zz0)
                to_mate(item, zz0)

        for hold, met, send in (
            (hold_left, lambda: pl.semaphore_wait(left_in, 1), lambda i, zz: onward(i, 1, zz)),
            (hold_twin, lambda: pl.semaphore_wait(twin_in, 1), to_twin),
            (hold_mate, lambda: pl.semaphore_wait(mate_in, 1), to_mate),
        ):
            @pl.when(hold & (k == defer))
            def _():
                if 3 not in items:
                    met()
                    if send is to_mate:
                        send_x()
                for s in range(defer + 1):
                    for item in items:
                        send(item, up(s))

    def begin(items):
        for item in items:
            onward(item, 0, z)

            @pl.when(jnp.logical_not(hold_left))
            def _():
                onward(item, 1, z)

            @pl.when(jnp.logical_not(hold_twin))
            def _():
                to_twin(item, z)

    def hand_over(k):
        @pl.when(has1(k))
        def _():
            ycopy(up(k), 1 - par).wait_recv()
            fcopy(up(k), c).start()

        @pl.when(has0(k))
        def _():
            ycopy(down(hop0(k)), 1 - par).wait_recv()
            fcopy(down(hop0(k)), c).start()

    def product(zz):
        both = wg.at[zz, :, 1 - c]
        remote(both, both, dsn.at[0], drc.at[zz], {"kv": twin}).wait_recv()
        xcopy(zz, R, R).wait_recv()
        x = xb[zz]
        return [
            jnp.dot(x, wg[zz, j].reshape(ZC, CW), preferred_element_type=F32) for j in range(3)
        ]

    def add_product(zz):
        for j, v in enumerate(product(zz)):
            acc[j] += v

    def products(k):
        @pl.when(has1(k))
        def _():
            add_product(up(k))

        @pl.when(has0(k))
        def _():
            add_product(down(hop0(k)))

    c0 = pl.multiple_of(par * CW, CW)
    mine = [
        pltpu.make_async_copy(src.at[:, pl.ds(c0, CW)], wg.at[z, i, c], loc.at[i])
        for i, src in enumerate((wq_h, wk_h, wv_h))
    ] + [
        pltpu.make_async_copy(wo_h.at[pl.ds(i * HO, HO), :], wo.at[z, c, i], loc.at[3 + i])
        for i in range(2)
    ]
    loads = [
        pltpu.make_async_copy(src, dst, loc.at[5 + i])
        for i, (src, dst) in enumerate((
            (tok_h, tok), (wig_h, wig), (wfg_h, wfg), (pk_h, pk), (pv_h, pv), (sn_h, sn), (st_h, st),
        ))
    ]
    barrier = pltpu.get_barrier_semaphore()

    def signal(sem, dev):
        pl.semaphore_signal(sem, inc=1, device_id=dev, device_id_type=MESH)

    right, left = lax.rem(tp + 1, TPN), lax.rem(tp + TPN - 1, TPN)
    tops, tops_l = tp < right, tp < left
    signal(barrier, {"kv": ring_to[1]})
    for cond, dev in (
        (c == 1, {"kv": twin}), (par == 1, {"grp": mate}),
        (jnp.logical_not(tops), {"tp": right}), (jnp.logical_not(tops_l), {"tp": left}),
    ):
        @pl.when(cond)
        def _():
            signal(barrier, dev)

    for cp in mine + loads:
        cp.start()
    for cp in mine:
        cp.wait()
    one = lambda cond: jnp.where(cond, 1, 0)
    pl.semaphore_wait(barrier, 1 + one(c == 0) + one(par == 0) + one(tops) + one(tops_l))
    signal(left_in, {"kv": ring_to[0]})
    for cond, sem, dev in (
        (c == 0, twin_in, {"kv": twin}), (par == 0, mate_in, {"grp": mate}),
        (tops, tp_in.at[0], {"tp": right}), (tops_l, tp_in.at[1], {"tp": left}),
    ):
        @pl.when(cond)
        def _():
            signal(sem, dev)

    @pl.when(jnp.logical_not(hold_left))
    def _():
        pl.semaphore_wait(left_in, 1)

    @pl.when((c == 1) & jnp.logical_not(hold_twin))
    def _():
        pl.semaphore_wait(twin_in, 1)

    @pl.when((par == 1) & jnp.logical_not(hold_mate))
    def _():
        pl.semaphore_wait(mate_in, 1)

    begin((0, 1, 2))

    loads[0].wait()
    g32[...] = ngain[...].astype(F32)
    h32[:HL] = hgain[...].astype(F32)
    xf[...] = jnp.zeros_like(xf)

    def norm_rows(t, carry):
        v = tok[t].astype(F32)
        xf[t, :B, :] = v * lax.rsqrt(jnp.mean(v * v, axis=-1, keepdims=True) + EPS)
        return carry

    lax.fori_loop(0, T, norm_rows, 0)
    LN = 128

    def cut_rows(i, carry):
        for j in range(ZC // LN):
            cols = pl.ds(pl.multiple_of(i * ZC + j * LN, LN), LN)
            v = xf[:, :, cols].reshape(R, LN) * g32[pl.ds(i * (ZC // LN) + j, 1), :]
            xb[i, :R, j * LN : (j + 1) * LN] = v.astype(BF16)
        return carry

    lax.fori_loop(0, NZ, cut_rows, 0)

    @pl.when(jnp.logical_not(hold_mate))
    def _():
        send_x()

    loads[1].wait()
    loads[2].wait()

    def gates(i, carry):
        a1, b0, b1 = carry
        cols = pl.ds(pl.multiple_of(i * ZC, ZC), ZC)
        xi, wi, wf = xb[i, :R, :], wig[:, cols], wfg[:, cols]
        dot = functools.partial(lax.dot_general, dimension_numbers=LAST, preferred_element_type=F32)
        return a1 + dot(xi, wf), b0 + dot(wi, xi), b1 + dot(wf, xi)

    zc_ = jnp.zeros((HL, R), F32)
    fr, ic, fc = lax.fori_loop(0, NZ, gates, (jnp.zeros((R, HL), F32), zc_, zc_))
    r0 = lax.broadcasted_iota(jnp.int32, (R, R), 0)
    r1 = lax.broadcasted_iota(jnp.int32, (R, R), 1)
    same = lax.rem(r0, BP) == lax.rem(r1, BP)
    upto = jnp.where(same & (r0 >= r1), 1.0, 0.0).astype(F32)
    cum_r = jnp.dot(
        upto, log_sigmoid(fr + fgb[...]), precision=HIGH, preferred_element_type=F32
    )
    lane_of = lambda ref: jnp.concatenate(
        [jnp.broadcast_to(ref[:, h : h + 1], (1, R)) for h in range(HL)], axis=0
    )
    cum_c = lax.dot_general(
        log_sigmoid(fc + lane_of(fgb)), upto, LAST, precision=HIGH, preferred_element_type=F32
    )
    gc[:HL, :] = ic + lane_of(igb) - cum_c

    lf, ig, run = [], [], None
    for t in range(T):
        live = t < acc_n[...]
        f = jnp.where(live, log_sigmoid(pfg[t]), 0.0)
        run = f if run is None else run + f
        lf.append(run)
        ig.append(jnp.where(live, pig[t], -1e30))
    wlog = [run - lf[t] + ig[t] for t in range(T)]
    top = functools.reduce(jnp.maximum, wlog)
    new_max = jnp.maximum(run + smax[...], top)
    nmax[...] = new_max
    eye = jnp.where(
        lax.broadcasted_iota(jnp.int32, (BP, B), 0) == lax.broadcasted_iota(jnp.int32, (BP, B), 1),
        1.0, 0.0,
    ).astype(F32)
    turn = lambda v: lax.dot_general(eye, v, LAST, precision=HIGH, preferred_element_type=F32)
    carry_r = turn(jnp.exp(run + smax[...] - new_max))
    max_r = turn(new_max)
    wts = [turn(jnp.exp(wlog[t] - new_max)) * (DK**-0.5) for t in range(T)]
    for h in range(HL):
        ab[h] = jnp.broadcast_to(carry_r[:, h : h + 1], (BP, DK))
        gr[h, 0] = jnp.broadcast_to(cum_r[:, h : h + 1], (R, DK))
        for t in range(T):
            gr[h, 1, t * BP : (t + 1) * BP] = jnp.broadcast_to(max_r[:, h : h + 1], (BP, DK))

    for cp in loads[3:6]:
        cp.wait()
    for ref in (kwb, vb, qb):
        ref[...] = jnp.zeros_like(ref)
    for h in range(HL):
        cols = slice(h * DK, (h + 1) * DK)
        total = None
        for t in range(T):
            kw = pk[t, :, cols].astype(F32) * wts[t][:B, h : h + 1]
            kwb[h, pl.ds(t, B, stride=8), :] = kw
            vb[h, pl.ds(t, B, stride=8), :] = pv[t, :, cols].astype(F32)
            total = kw if total is None else total + kw
        nrm[h, :B] = total
    for b in range(B):
        for h in range(HL):
            row = ab[h, b : b + 1] * sn[b, h : h + 1] + nrm[h, b : b + 1]
            nrm[h, b : b + 1] = row
            nnorm[b, h : h + 1] = row
    loads[6].wait()

    def fold(b):
        rows = pl.ds(pl.multiple_of(b * 8, 8), 8)
        for h in range(HL):
            outer = lax.dot_general(
                kwb[h, rows, :].astype(BF16), vb[h, rows, :].astype(BF16),
                (((0,), (0,)), ((), ())), preferred_element_type=F32,
            )
            s = st[b, h] * ab[h, pl.ds(b, 1), :] + outer
            st[b, h] = s
            sb[b, h] = s.astype(BF16)

    per = B // SLOTS
    for b in range(per * SLOTS, B):
        fold(b)

    acc[...] = jnp.zeros_like(acc)

    @pl.when(jnp.logical_not(hold_sum))
    def _():
        add_product(z)

    def ring(k, carry):
        arrive((0, 1, 2), k, LATE)

        @pl.when(k == LAG)
        def _():
            begin((3,))

        arrive((3,), k - LAG, LATE - LAG)

        @pl.when(jnp.logical_not(hold_sum) | (k > LATE + 1))
        def _():
            products(k - 1)

        @pl.when(hold_sum & (k == LATE + 1))
        def _():
            lax.fori_loop(0, LATE + 1, lambda s, c_: (add_product(up(s)), c_)[1], 0)

        for i in range(per):
            fold((k - 1) * per + i)
        return carry

    lax.fori_loop(1, SLOTS + 1, ring, 0)
    products(SLOTS)

    def qcopy(j, i, half):
        cols = pl.ds(i * DK, DK)
        return remote(
            sendq.at[j, :, cols], qall.at[j, half, :, cols], qs_sem.at[j, i], qr_sem.at[j, i],
            {"grp": mate},
        )

    for i in range(2):
        for j in range(3):
            cols = slice(i * DK, (i + 1) * DK)
            sendq[j, :, cols] = acc[j, R:, cols].astype(BF16)
            qcopy(j, i, par).start()
    for j in range(3):
        qall[j, par] = acc[j, :R].astype(BF16)

    def out_slot(k):
        arrive((3,), jnp.int32(k - LAG), LATE - LAG)

    keep = same & (r0 >= r1) & (lax.rem(r1, BP) < B)

    def spread(half, i):
        h = half * 2 + i
        q = qall[0, half, :, i * DK : (i + 1) * DK].astype(F32)
        for t in range(T):
            qb[h, pl.ds(t, BP, stride=8), :] = q[t * BP : (t + 1) * BP]
        for b in range(B):
            rows = slice(b * 8, b * 8 + 8)
            qsb[h, rows, :] = jnp.dot(
                qb[h, rows, :].astype(BF16), sb[b, h], preferred_element_type=F32
            )

    def head(half, i):
        h = half * 2 + i
        cols = slice(i * DK, (i + 1) * DK)
        q, k, v = (qall[j, half, :, cols] for j in range(3))
        cum = gr[h, 0, :, :1]
        inter = cum + gr[h, 1, :, :1]
        decay = jnp.where(keep, cum + gc[pl.ds(h, 1), :], -1e30)
        top_r = jnp.maximum(inter, jnp.max(decay, axis=1, keepdims=True))
        scale = jnp.exp(inter - top_r)
        scores = lax.dot_general(q, k, LAST, preferred_element_type=F32) * (DK**-0.5)
        scores = scores * jnp.exp(decay - top_r)
        q32 = q.astype(F32)
        nh = nrm[h]
        read = jnp.concatenate(
            [qsb[h, pl.ds(t, BP, stride=8), :] for t in range(T)], axis=0
        )
        qn = jnp.concatenate(
            [
                jnp.sum(q32[t * BP : (t + 1) * BP] * nh, axis=1, keepdims=True)
                for t in range(T)
            ],
            axis=0,
        )
        num = scale * read + jnp.dot(scores.astype(BF16), v, preferred_element_type=F32)
        den = scale * qn + jnp.sum(scores, axis=1, keepdims=True)
        cell = num / jnp.maximum(jnp.abs(den), jnp.exp(-top_r))
        cell = cell * lax.rsqrt(jnp.mean(cell * cell, axis=1, keepdims=True) + EPS)
        hc = pl.ds(pl.multiple_of(h * DK, DK), DK)
        hid[:, hc] = (cell * h32[pl.ds(h, 1), :]).astype(BF16)

    nrm[:, B:] = jnp.zeros((HL, BP - B, DK), F32)
    qsb[:, B * 8 :, :] = jnp.zeros((HL, (BP - B) * 8, DK), F32)
    def handed(lo, hi):
        def one_slot(k, carry):
            hand_over(k)
            return carry

        lax.fori_loop(lo, hi, one_slot, 0)

    steps = [
        lambda: (spread(par, 0), spread(par, 1)), lambda: head(par, 0), lambda: head(par, 1),
    ]
    for i in range(LAG):
        with jax.named_scope("outslot"):
            out_slot(SLOTS + 1 + i)
        if i < len(steps):
            steps[i]()
    for f in steps[LAG:]:
        f()
    handed(1, 5)
    for i in range(2):
        with jax.named_scope("qwait"):
            for j in range(3):
                qcopy(j, i, par).wait_send()
                qcopy(j, i, 1 - par).wait_recv()
        spread(1 - par, i)
        head(1 - par, i)
    with jax.named_scope("handed"):
        handed(5, SLOTS + 1)
    for half, sem in ((par, drw), (1 - par, fr_sem)):
        ref = wo.at[:, 1 - c, half]
        remote(ref, ref, fs, sem, {"kv": twin}).wait_recv()

    @pl.when(jnp.logical_not(tops))
    def _():
        pl.semaphore_wait(tp_in.at[1], 1)

    @pl.when(jnp.logical_not(tops_l))
    def _():
        pl.semaphore_wait(tp_in.at[0], 1)

    per_tp = NZ // TPN
    NB = CORES * OC
    HW = per_tp * NB // 2

    def block(target, i):
        zz = target * per_tp + i
        w = jnp.concatenate(
            [wo[zz, cc].reshape(2 * HO, OC) for cc in range(CORES)], axis=1
        )
        return jnp.dot(hid[...], w, preferred_element_type=F32)

    def chunk(target, half):
        n = per_tp // 2
        return jnp.concatenate([block(target, half * n + i) for i in range(n)], axis=1)

    def rcopy(i):
        return remote(
            rout.at[i], rin.at[i], rs_sem.at[i], rr_sem.at[i],
            {"tp": right if i % 2 == 0 else left},
        )

    far = lax.rem(tp + 2, TPN)
    for i, (target, half) in enumerate(((far, 0), (far, 1), (right, 1), (left, 0))):
        rout[i] = chunk(target, half).astype(BF16)
        rcopy(i).start()
    part[0] = chunk(right, 0)
    part[1] = chunk(left, 1)
    for i in range(2):
        rcopy(i).wait_recv()
        rout[4 + i] = (part[i] + rin[i].astype(F32)).astype(BF16)
        rcopy(4 + i).start()
    for i in range(2):
        part[i] = chunk(tp, i)

    def sent(ref, sem):
        remote(ref, ref, sem, drw, {"kv": twin}).wait_send()

    for item in range(4):
        kind = lambda n: wg.at[pl.ds(0, n), item, 0] if item < 3 else wo.at[pl.ds(0, n), 0, 0]
        sent(kind(N0), zs.at[item, 0])
        sent(kind(N1), zs.at[item, 1])
        sent(kind(NZ), dsn.at[item])
    sent(wo.at[pl.ds(0, NZ - 1), 0, 0], ys)
    sent(wo.at[pl.ds(0, NZ), 0, 0], fs)
    sent(xb.at[:, pl.ds(0, R), :], xs)
    for i in range(6):
        rcopy(i).wait_send()
        if i >= 2:
            rcopy(i).wait_recv()
    for t in range(T):
        rows = slice(t * BP, (t + 1) * BP)
        lo = part[0, rows] + rin[4, rows].astype(F32) + rin[3, rows].astype(F32)
        hi = part[1, rows] + rin[2, rows].astype(F32) + rin[5, rows].astype(F32)
        mixed[t, :, :HW] = lo[:B]
        mixed[t, :, HW:] = hi[:B]


def hand_out(mixed_i, nmat_i, nnorm_i, nmax_i, mixed_o, nmat_o, nnorm_o, nmax_o, sems):
    n = nmat_i.shape[0] // 2
    pairs = [(nmat_i.at[pl.ds(i * n, n)], nmat_o.at[pl.ds(i * n, n)]) for i in range(2)]
    pairs += [(mixed_i, mixed_o), (nnorm_i, nnorm_o), (nmax_i, nmax_o)]
    copies = [pltpu.make_async_copy(a, b, sems.at[i]) for i, (a, b) in enumerate(pairs)]
    for cp in copies:
        cp.start()
    for cp in copies:
        cp.wait()


def body(
    tokens, norm_gain, w_query, w_key, w_value, w_igate, w_fgate, igate_bias, fgate_bias,
    head_gain, w_out, state_matrix, state_norm, state_max, prior_keys, prior_values,
    prior_igate, prior_fgate, accepted,
):
    B, T, D = tokens.shape
    HL, DK = state_matrix.shape[1:3]
    NZ = lax.axis_size("kv") // CORES
    TPN = lax.axis_size("tp")
    BP = -(-B // 8) * 8
    R = T * BP
    W = w_query.shape[1]
    CW = W // 2
    KC = w_query.shape[0]
    ZC = KC * CORES
    OC = w_out.shape[1]
    OW = D // TPN
    VM = pl.BlockSpec(memory_space=pltpu.VMEM)
    HB = pl.BlockSpec(memory_space=pl.ANY)
    V, DMA, REG = pltpu.VMEM, pltpu.SemaphoreType.DMA, pltpu.SemaphoreType.REGULAR
    shapes = (
        jax.ShapeDtypeStruct((T, B, OW), F32),
        jax.ShapeDtypeStruct(state_matrix.shape, F32),
        jax.ShapeDtypeStruct(state_norm.shape, F32),
        jax.ShapeDtypeStruct((HL, B), F32),
    )
    outs = pl.pallas_call(
        functools.partial(kernel, (B, T, BP, NZ, TPN, HL, DK)),
        out_shape=tuple(V(a.shape, a.dtype) for a in shapes),
        in_specs=[HB, VM, HB, HB, HB, HB, HB, VM, VM, VM, HB, HB, HB, VM, HB, HB, VM, VM, VM],
        out_specs=(VM, VM, VM, VM),
        scratch_shapes=[
            V((T, B, D), BF16), V((T, BP, D), F32), V((NZ, 2 * R, ZC), BF16),
            V((NZ, 3, CORES, KC, CW), BF16), V((NZ, CORES, 2, W // 2, OC), BF16),
            V((3, 2 * R, CW), F32),
            V(state_matrix.shape, BF16),
            V((T, B, W), BF16), V((T, B, W), BF16), V(state_norm.shape, F32),
            V((HL, D), BF16), V((HL, D), BF16),
            V((HL, BP * 8, DK), F32), V((HL, BP * 8, DK), F32),
            V((HL, BP * 8, DK), F32), V((HL, BP * 8, DK), F32),
            V((HL, 2, R, DK), F32), V((8, R), F32), V((HL, BP, DK), F32), V((HL, BP, DK), F32),
            V((D // 128, 128), F32), V((8, DK), F32),
            V((3, 2, R, CW), BF16), V((3, R, CW), BF16), V((R, W), BF16),
            V((6, R, OW // 2), BF16), V((6, R, OW // 2), BF16), V((2, R, OW // 2), F32),
            DMA((12,)), DMA((4, 2)), DMA((4, NZ)), DMA((4,)), DMA((NZ,)), DMA,
            DMA, DMA((NZ,)), DMA, DMA((NZ,)), DMA, DMA,
            DMA((3, 2)), DMA((3, 2)), DMA((6,)), DMA((6,)),
            REG, REG, REG, pltpu.SemaphoreType.REGULAR((2,)),
        ],
        compiler_params=pltpu.CompilerParams(
            collective_id=0, has_side_effects=True, vmem_limit_bytes=56 * 1024 * 1024
        ),
        name="cell",
    )(
        tokens.transpose(1, 0, 2), norm_gain.reshape(-1, 128), w_query, w_key, w_value,
        w_igate.T, w_fgate.T, igate_bias.reshape(1, -1), fgate_bias.reshape(1, -1),
        head_gain.reshape(-1, DK), w_out, state_matrix, state_norm, state_max.T,
        prior_keys.transpose(1, 0, 2), prior_values.transpose(1, 0, 2),
        prior_igate.transpose(1, 2, 0), prior_fgate.transpose(1, 2, 0), accepted.reshape(1, -1),
    )
    mixed, new_matrix, new_norm, new_max = pl.pallas_call(
        hand_out, out_shape=shapes, in_specs=[VM] * 4, out_specs=(HB,) * 4,
        scratch_shapes=[DMA((5,))], name="hand_out",
        compiler_params=pltpu.CompilerParams(vmem_limit_bytes=56 * 1024 * 1024),
    )(*(pltpu.with_memory_space_constraint(a, pltpu.VMEM) for a in outs))
    return mixed.transpose(1, 0, 2), new_matrix, new_norm, new_max.T


def solution(mesh):
    rows = ("grp", "kv")
    return jax.shard_map(
        body,
        mesh=mesh,
        in_specs=(
            P(rows, None, None), P(), P("kv", "tp"), P("kv", "tp"), P("kv", "tp"),
            P(None, "tp"), P(None, "tp"), P("tp"), P("tp"), P("tp"), P("tp", "kv"),
            P(rows, "tp", None, None), P(rows, "tp", None), P(rows, "tp"),
            P(rows, None, "tp"), P(rows, None, "tp"), P(rows, None, "tp"), P(rows, None, "tp"),
            P(rows),
        ),
        out_specs=(
            P(rows, None, "tp"), P(rows, "tp", None, None), P(rows, "tp", None), P(rows, "tp"),
        ),
        check_vma=False,
    )
```
